32 devices in a mesh: sp: 16 (over z, y, x), tp: 2 (over core).
Axes of the slice: x: 2, y: 2, z: 4, core: 2. Of those that a mesh axis runs over, the one named last changes fastest.
Arguments:
- tokens: bfloat16 [6144, 2048], P('sp', 'tp'), may hold values from -40 to 40
- mix_gain: float32 [2048], replicated, may hold values from 0.1 to 1.9
- w_pool_in: bfloat16 [2048, 1024], P(None, 'tp'), may hold values from -0.125 to 0.125
- w_qlat: bfloat16 [2048, 512], P(None, 'tp'), may hold values from -0.125 to 0.125
- w_kvlat: bfloat16 [2048, 512], P(None, 'tp'), may hold values from -0.125 to 0.125
- w_krope: bfloat16 [2048, 64], replicated, may hold values from -0.125 to 0.125
- q_gain: float32 [512], replicated, may hold values from 1 to 60
- kv_gain: float32 [512], replicated, may hold values from 0.1 to 1.9
- w_q_content: bfloat16 [512, 2048], P(None, 'tp'), may hold values from -0.25 to 0.25
- w_q_rotary: bfloat16 [512, 1024], P(None, 'tp'), may hold values from -0.25 to 0.25
- w_key: bfloat16 [512, 2048], P(None, 'tp'), may hold values from -0.25 to 0.25
- w_value: bfloat16 [512, 2048], P(None, 'tp'), may hold values from -0.25 to 0.25
- pool_mix: bfloat16 [8, 128, 128], replicated, may hold values from -0.5 to 0.5
- pool_scale: float32 [1024], replicated, may hold values from 0.1 to 1.9
- w_out_pool: bfloat16 [1024, 2048], P('tp'), may hold values from -0.109375 to 0.109375
- w_out_attn: bfloat16 [2048, 2048], P('tp'), may hold values from -0.25 to 0.25
Outputs:
- layer_out: bfloat16 [6144, 2048], P(('sp', 'tp'))
- log_total: float32 [6144, 16], P('sp', 'tp')
The draws below stay inside these ranges and needn't reach their ends.
All inputs are finite; a program needn't handle non-finite values.
Results may differ from the reference program's by a relative error of at most 0.015.
The reference program's roundings to bfloat16 on the way (of `scaled`, `weights`, `attended`, `pooled` and `pool_out`) count: a program that leaves them out, or rounds other values in their place, can miss the bound.
Values may be sent and summed in bfloat16 or wider, within the bound.
No kernel may reach another device: no remote copies, remote signals or barrier semaphores. Data moves between devices by JAX's collectives and lax.ppermute only.
A program may use at most 64 MiB of HBM per device.

```python
import jax
import jax.numpy as jnp
from jax import lax

D = 2048
HEADS = 16
NOPE = 128
ROPE = 64
VDIM = 128
QLAT = 512
KVLAT = 512
GROUPS = 8
GROUP_DIM = 128
WIDEST = 16
SPAN = 16
TOK_DEV = 384
POOL = 1024
MIX = 3072
SEQ_LEN = 6144
SEQS = 1
TOKENS = 6144


def draw_tokens(key, part):
    base_key, column_key = jax.random.split(jax.random.fold_in(key, 11), 2)
    base = jnp.clip(jax.random.normal(base_key, (TOKENS, D), jnp.float32), -6.0, 6.0)
    ramp = jnp.arange(D, dtype=jnp.float32) / D
    column_scale = jnp.exp(jnp.log(4.0) * ramp + jax.random.uniform(column_key, (D,), jnp.float32, -0.5, 0.5))
    return jnp.clip(base * column_scale[None, :], -40.0, 40.0).astype(jnp.bfloat16)


def draw_q_gain(key, part):
    gain_key = jax.random.fold_in(key, 23)
    logs = jax.random.uniform(gain_key, (QLAT,), jnp.float32, 0.0, jnp.log(4.0))
    return jnp.exp(logs)


def steps_of(own_key, shape, cuts, least, high):
    gain, own = 1.0, jax.random.fold_in(own_key, 6)
    for axis_at, parts in cuts:
        heights = jnp.exp(jax.random.uniform(jax.random.fold_in(own, axis_at), (parts,), jnp.float32, least / len(cuts), high / len(cuts)))
        gain = gain * jnp.repeat(heights, shape[axis_at] // parts).reshape([-1 if axis == axis_at else 1 for axis in range(len(shape))])
    return gain


def normal_values(key, extent, spread, most, shards=(), kind=jnp.bfloat16):
    drawn = jax.random.normal(key, extent, jnp.float32) * spread
    if len(shards) > 0:
        drawn = steps_of(key, extent, shards, -0.22, 0.18) * drawn
    return jnp.clip(drawn, min=-most, max=most).astype(kind)


def setup_inputs(seed: int = 0) -> dict:
    keys = jax.random.split(jax.random.key(seed), 17)
    tokens = draw_tokens(jax.random.fold_in(keys[16], 71), 0)
    mix_gain = jnp.clip(1.0 + 0.18 * jax.random.normal(keys[1], (D,), jnp.float32), 0.1, 1.9)
    w_pool_in = normal_values(keys[2], (D, POOL), D ** -0.5, 0.125, ((1, 2),))
    w_qlat = normal_values(keys[3], (D, QLAT), D ** -0.5, 0.125, ((1, 2),))
    w_kvlat = normal_values(keys[4], (D, KVLAT), D ** -0.5, 0.125, ((1, 2),))
    w_krope = normal_values(keys[5], (D, ROPE), D ** -0.5, 0.125)
    q_gain = draw_q_gain(jax.random.fold_in(keys[16], 71), 0)
    kv_gain = jnp.clip(1.0 + 0.18 * jax.random.normal(keys[7], (KVLAT,), jnp.float32), 0.1, 1.9)
    w_q_content = normal_values(keys[8], (QLAT, HEADS * NOPE), QLAT ** -0.5, 0.25, ((1, 2),))
    w_q_rotary = normal_values(keys[9], (QLAT, HEADS * ROPE), QLAT ** -0.5, 0.25, ((1, 2),))
    w_key = normal_values(keys[10], (KVLAT, HEADS * NOPE), KVLAT ** -0.5, 0.25, ((1, 2),))
    w_value = normal_values(keys[11], (KVLAT, HEADS * VDIM), KVLAT ** -0.5, 0.25, ((1, 2),))
    pool_mix = normal_values(keys[12], (GROUPS, GROUP_DIM, GROUP_DIM), GROUP_DIM ** -0.5, 0.5)
    pool_scale = jnp.clip(1.0 + 0.18 * jax.random.normal(keys[13], (POOL,), jnp.float32), 0.1, 1.9)
    w_out_pool = normal_values(keys[14], (POOL, D), MIX ** -0.5, 0.109375, ((0, 2),))
    w_out_attn = normal_values(keys[15], (HEADS * VDIM, D), (HEADS * VDIM // 4) ** -0.5, 0.25, ((0, 2),))
    return {"tokens": tokens, "mix_gain": mix_gain, "w_pool_in": w_pool_in, "w_qlat": w_qlat, "w_kvlat": w_kvlat, "w_krope": w_krope, "q_gain": q_gain, "kv_gain": kv_gain, "w_q_content": w_q_content, "w_q_rotary": w_q_rotary, "w_key": w_key, "w_value": w_value, "pool_mix": pool_mix, "pool_scale": pool_scale, "w_out_pool": w_out_pool, "w_out_attn": w_out_attn}


eps_norm = 1e-06
rope_base = 10000.0
masked_score = -1e+30

def tables(positions, rotary_width):
    half_width = rotary_width // 2
    frequency = rope_base ** (-jnp.arange(half_width, dtype=jnp.float32) * 2.0 / rotary_width)
    angles = positions.astype(jnp.float32)[:, None] * frequency[None, :]
    return (jnp.cos(angles), jnp.sin(angles))

def rotate(vectors, cosine, sine_table):
    half_width = vectors.shape[-1] // 2
    first_half = vectors[..., :half_width]
    second_half = vectors[..., half_width:]
    return jnp.concatenate([first_half * cosine - second_half * sine_table, second_half * cosine + first_half * sine_table], axis=-1)

def latent_norm(latent, gain_vector):
    latent_values = latent.astype(jnp.float32)
    inverse = lax.rsqrt(lax.optimization_barrier(jnp.mean(latent_values * latent_values, axis=-1, keepdims=True)) + eps_norm)
    return (latent_values * inverse * gain_vector).astype(jnp.bfloat16)

def one_sequence(seq_tokens, mix_gain, w_pool_in, w_qlat, w_kvlat, w_krope, q_gain, kv_gain, w_q_content, w_q_rotary, w_key, w_value, pool_mix, pool_scale, w_out_pool, w_out_attn):
    length = seq_tokens.shape[0]
    positions = jnp.arange(length, dtype=jnp.int32)
    raw_values = seq_tokens.astype(jnp.float32)
    inverse_rms = lax.rsqrt(lax.optimization_barrier(jnp.mean(raw_values * raw_values, axis=1, keepdims=True)) + eps_norm)
    scaled = (raw_values * mix_gain).astype(jnp.bfloat16)

    def project(weight):
        return (jnp.dot(scaled, weight, preferred_element_type=jnp.float32) * inverse_rms).astype(jnp.bfloat16)
    pool_pre = project(w_pool_in)
    query_latent = project(w_qlat)
    kv_latent = project(w_kvlat)
    rotary_raw = project(w_krope)
    query_normed = latent_norm(query_latent, q_gain)
    key_normed = latent_norm(kv_latent, kv_gain)
    cosine, sine_table = tables(positions, ROPE)
    query_content = jnp.dot(query_normed, w_q_content, preferred_element_type=jnp.float32).astype(jnp.bfloat16).reshape(length, HEADS, NOPE)
    key_content = jnp.dot(key_normed, w_key, preferred_element_type=jnp.float32).astype(jnp.bfloat16).reshape(length, HEADS, NOPE)
    values = jnp.dot(key_normed, w_value, preferred_element_type=jnp.float32).astype(jnp.bfloat16).reshape(length, HEADS, VDIM)
    query_rotary = rotate(jnp.dot(query_normed, w_q_rotary, preferred_element_type=jnp.float32).reshape(length, HEADS, ROPE), cosine[:, None, :], sine_table[:, None, :]).astype(jnp.bfloat16)
    key_rotary = rotate(rotary_raw.astype(jnp.float32), cosine, sine_table).astype(jnp.bfloat16)
    score_scale = (NOPE + ROPE) ** (-0.5)
    key_content_wide = key_content.astype(jnp.float32)
    key_rotary_wide = key_rotary.astype(jnp.float32)
    values_wide = values.astype(jnp.float32)

    def query_block(block_index):
        row_start = block_index * TOK_DEV
        block_content = lax.dynamic_slice_in_dim(query_content, row_start, TOK_DEV, 0).astype(jnp.float32)
        block_rotary = lax.dynamic_slice_in_dim(query_rotary, row_start, TOK_DEV, 0).astype(jnp.float32)
        scores = jnp.einsum('qhd,khd->qhk', block_content, key_content_wide, precision=lax.Precision.HIGHEST)
        scores = scores + jnp.einsum('qhr,kr->qhk', block_rotary, key_rotary_wide, precision=lax.Precision.HIGHEST)
        query_positions = row_start + jnp.arange(TOK_DEV, dtype=jnp.int32)
        allowed = positions[None, None, :] <= query_positions[:, None, None]
        scores = jnp.where(allowed, scores * score_scale, masked_score)
        row_max = lax.optimization_barrier(jnp.max(scores, axis=-1))
        expo = jnp.exp(scores - row_max[..., None])
        row_total = lax.optimization_barrier(jnp.sum(expo, axis=-1))
        weights = lax.optimization_barrier(expo.astype(jnp.bfloat16))
        summed = jnp.einsum('qhk,khd->qhd', weights.astype(jnp.float32), values_wide, precision=lax.Precision.HIGHEST)
        attended = (summed / row_total[..., None]).astype(jnp.bfloat16).reshape(TOK_DEV, HEADS * VDIM)
        return (attended, row_max + jnp.log(row_total))
    attended, log_total = lax.map(query_block, jnp.arange(length // TOK_DEV))
    attended = attended.reshape(length, HEADS * VDIM)
    log_total = log_total.reshape(length, HEADS)
    pool_values = pool_pre.astype(jnp.float32)
    extended = jnp.concatenate([jnp.zeros((WIDEST - 1, POOL), jnp.float32), pool_values], axis=0)
    groups = jnp.arange(POOL, dtype=jnp.int32) // GROUP_DIM
    windows = jnp.left_shift(jnp.int32(2), groups % 4)
    window_sums = jnp.zeros((length, POOL), jnp.float32)
    for distance in range(WIDEST):
        window_sums = window_sums + jnp.where(distance < windows[None, :], extended[WIDEST - 1 - distance:WIDEST - 1 - distance + length], 0.0)
    counts = jnp.minimum(positions[:, None] + 1, windows[None, :]).astype(jnp.float32)
    pooled = lax.optimization_barrier((window_sums / counts - pool_values).astype(jnp.bfloat16))
    mixed_pool = jnp.einsum('sgc,gcd->sgd', pooled.astype(jnp.float32).reshape(length, GROUPS, GROUP_DIM), pool_mix.astype(jnp.float32), precision=lax.Precision.HIGHEST).reshape(length, POOL)
    pool_out = (mixed_pool * pool_scale).astype(jnp.bfloat16)
    layer_out = jnp.dot(pool_out, w_out_pool, preferred_element_type=jnp.float32)
    layer_out = layer_out + jnp.dot(attended, w_out_attn, preferred_element_type=jnp.float32)
    return (layer_out.astype(jnp.bfloat16), log_total)

def reference(tokens, mix_gain, w_pool_in, w_qlat, w_kvlat, w_krope, q_gain, kv_gain, w_q_content, w_q_rotary, w_key, w_value, pool_mix, pool_scale, w_out_pool, w_out_attn):
    sequences = tokens.reshape(SPAN, SEQS, TOK_DEV, D).transpose(1, 0, 2, 3).reshape(SEQS, SEQ_LEN, D)

    def per_sequence(seq_tokens):
        return one_sequence(seq_tokens, mix_gain, w_pool_in, w_qlat, w_kvlat, w_krope, q_gain, kv_gain, w_q_content, w_q_rotary, w_key, w_value, pool_mix, pool_scale, w_out_pool, w_out_attn)
    outputs, log_sums = lax.map(per_sequence, sequences)
    outputs = outputs.reshape(SEQS, SPAN, TOK_DEV, D).transpose(1, 0, 2, 3).reshape(TOKENS, D)
    log_sums = log_sums.reshape(SEQS, SPAN, TOK_DEV, HEADS).transpose(1, 0, 2, 3).reshape(TOKENS, HEADS)
    return (outputs, log_sums)
```

```python
import functools

import jax
import jax.numpy as jnp
from jax import lax
from jax.experimental import pallas as pl
from jax.experimental.pallas import tpu as pltpu
from jax.sharding import PartitionSpec as P

NOPE = 128
ROPE = 64
VDIM = 128
GROUP_DIM = 128
WIDEST = 16
SPAN = 16
PLANE = 4

eps_norm = 1e-06
rope_base = 10000.0
masked_score = -1e30
log2e = 1.4426950408889634


def swap_tp(value):
    return lax.ppermute(value, "tp", [(0, 1), (1, 0)])


def shifted(value, axis, pairs):
    return lax.ppermute(value, axis, pairs)


def tables(positions, rotary_width):
    half_width = rotary_width // 2
    frequency = rope_base ** (-jnp.arange(half_width, dtype=jnp.float32) * 2.0 / rotary_width)
    angles = positions.astype(jnp.float32)[:, None] * frequency[None, :]
    return (jnp.cos(angles), jnp.sin(angles))


def attn_body(*refs, groups, part_count, heads, first, last, diagonal, scale):
    refs = list(refs)
    flags = refs.pop(0)
    q_ref = refs.pop(0)
    wk = [refs.pop(0) for _ in range(part_count)]
    wv = [refs.pop(0) for _ in range(part_count)]
    block_count = sum(len(group) for group in groups)
    blocks = [[refs.pop(0) for _ in range(part_count)] for _ in range(block_count)]
    if not first:
        max_in, sum_in, acc_in = refs.pop(0), refs.pop(0), refs.pop(0)
    if last:
        out_ref, log_ref = refs.pop(0), refs.pop(0)
        max_ref, sum_ref, acc_ref = refs.pop(0), refs.pop(0), refs.pop(0)
    else:
        max_ref, sum_ref, acc_ref = refs.pop(0), refs.pop(0), refs.pop(0)
    kt_ref, vt_ref = refs.pop(0), refs.pop(0)
    rows = q_ref.shape[1]
    keys = blocks[0][0].shape[1]
    factor = scale * log2e

    if first:
        max_ref[...] = jnp.full(max_ref.shape, masked_score, jnp.float32)
        sum_ref[...] = jnp.zeros(sum_ref.shape, jnp.float32)
        acc_ref[...] = jnp.zeros(acc_ref.shape, jnp.float32)
    else:
        max_ref[...] = max_in[...]
        sum_ref[...] = sum_in[...]
        acc_ref[...] = acc_in[...]

    def project(block, at):
        channels = wk[0].shape[1]
        span = slice(at * keys, (at + 1) * keys)
        k_rows = None
        v_rows = None
        for part in range(part_count):
            piece = block[part][:channels, :]
            k_part = jnp.dot(wk[part][...], piece, preferred_element_type=jnp.float32)
            v_part = jnp.dot(wv[part][...], piece, preferred_element_type=jnp.float32)
            k_rows = k_part if k_rows is None else k_rows + k_part
            v_rows = v_part if v_rows is None else v_rows + v_part
        vt_ref[:, span] = v_rows.astype(jnp.bfloat16)
        k_rows = k_rows.astype(jnp.bfloat16)
        rot_rows = block[0].shape[0] - channels
        for head in range(heads):
            kt_ref[head, :NOPE, span] = k_rows[head * NOPE : (head + 1) * NOPE]
            for part in range(part_count):
                low = NOPE + part * rot_rows
                kt_ref[head, low : low + rot_rows, span] = block[part][channels:, :]

    def softmax_group(width, masked):
        for head in range(heads):
            scores = jnp.dot(
                q_ref[head], kt_ref[head, :, :width], preferred_element_type=jnp.float32
            )
            if masked:
                row = lax.broadcasted_iota(jnp.int32, scores.shape, 0)
                col = lax.broadcasted_iota(jnp.int32, scores.shape, 1)
                scores = jnp.where(col <= row, scores, masked_score)
            old = max_ref[head]
            new = jnp.maximum(old, jnp.max(scores, axis=1, keepdims=True))
            shrink = jnp.exp2((old - new) * factor)
            total = sum_ref[head] * shrink
            tiles = []
            for tile in range(width // 128):
                expo = jnp.exp2((scores[:, tile * 128 : (tile + 1) * 128] - new) * factor)
                total = total + expo
                tiles.append(expo.astype(jnp.bfloat16))
            weights = jnp.concatenate(tiles, axis=1)
            max_ref[head] = new
            sum_ref[head] = total
            acc_ref[head] = acc_ref[head] * shrink + lax.dot_general(
                weights,
                vt_ref[head * VDIM : (head + 1) * VDIM, :width],
                (((1,), (1,)), ((), ())),
                preferred_element_type=jnp.float32,
            )

    at = 0
    for index, group in enumerate(groups):
        members = blocks[at : at + len(group)]
        at += len(group)

        def work(members=members):
            for slot, block in enumerate(members):
                project(block, slot)
            softmax_group(len(members) * keys, diagonal)

        if diagonal:
            work()
        else:
            pl.when(flags[index] != 0)(work)

    if last:
        for head in range(heads):
            total = jnp.sum(sum_ref[head], axis=1, keepdims=True)
            out_ref[:, head * VDIM : (head + 1) * VDIM] = (acc_ref[head] / total).astype(
                jnp.bfloat16
            )
            log_ref[:, head : head + 1] = max_ref[head][:, :1] * scale + jnp.log(total)


def attn_call(flags, queries, wk, wv, blocks, groups, state, last, diagonal, scale):
    heads, rows, depth = queries.shape
    first = state is None
    keys = blocks[0][0].shape[1]
    widest = max(len(group) for group in groups) * keys
    body = functools.partial(
        attn_body,
        groups=groups,
        part_count=len(wk),
        heads=heads,
        first=first,
        last=last,
        diagonal=diagonal,
        scale=scale,
    )
    operands = [flags, queries, *wk, *wv]
    for block in blocks:
        operands.extend(block)
    vmem = pl.BlockSpec(memory_space=pltpu.VMEM)
    in_specs = [pl.BlockSpec(memory_space=pltpu.SMEM)] + [vmem] * (len(operands) - 1)
    state_shapes = [jax.ShapeDtypeStruct((heads, rows, 128), jnp.float32)] * 2 + [
        jax.ShapeDtypeStruct((heads, rows, VDIM), jnp.float32)
    ]
    aliases = {}
    if not first:
        if not last:
            aliases = {len(operands) + i: i for i in range(3)}
        operands.extend(state)
        in_specs.extend([vmem] * 3)
    scratch = [
        pltpu.VMEM((heads, NOPE + ROPE, widest), jnp.bfloat16),
        pltpu.VMEM((heads * VDIM, widest), jnp.bfloat16),
    ]
    if last:
        out_shape = [
            jax.ShapeDtypeStruct((rows, heads * VDIM), jnp.bfloat16),
            jax.ShapeDtypeStruct((rows, heads), jnp.float32),
        ]
        scratch = [pltpu.VMEM(s.shape, s.dtype) for s in state_shapes] + scratch
    else:
        out_shape = state_shapes
    flops = sum(len(group) for group in groups) * keys * heads * 2
    flops = flops * (rows * (NOPE + ROPE + VDIM) + (NOPE + VDIM) * 512)
    return pl.pallas_call(
        body,
        out_shape=out_shape,
        in_specs=in_specs,
        out_specs=[vmem] * len(out_shape),
        scratch_shapes=scratch,
        input_output_aliases=aliases,
        compiler_params=pltpu.CompilerParams(vmem_limit_bytes=40 * 1024 * 1024),
        cost_estimate=pl.CostEstimate(
            flops=flops, bytes_accessed=20 * 1024 * 1024, transcendentals=flops // 600
        ),
    )(*operands)


def per_device(
    tokens,
    mix_gain,
    w_pool_in,
    w_qlat,
    w_kvlat,
    w_krope,
    q_gain,
    kv_gain,
    w_q_content,
    w_q_rotary,
    w_key,
    w_value,
    pool_mix,
    pool_scale,
    w_out_pool,
    w_out_attn,
):
    tp_size = lax.axis_size("tp")
    tp_rank = lax.axis_index("tp")
    sp_size = lax.axis_size("sp")
    sp_rank = lax.axis_index("sp")
    seq_count = sp_size // SPAN
    local_rows, own_width = tokens.shape
    model_width = own_width * tp_size
    seq_rank = sp_rank // seq_count
    pool_cols = w_pool_in.shape[1]
    query_cols = w_qlat.shape[1]
    latent_cols = w_kvlat.shape[1]
    own_heads = w_key.shape[1] // NOPE
    half = ROPE // 2
    pair = tp_size == 2

    def ordered(own, other, axis):
        return jnp.where(
            tp_rank == 0,
            jnp.concatenate([own, other], axis=axis),
            jnp.concatenate([other, own], axis=axis),
        )

    def gathered(value, axis):
        if pair:
            return ordered(value, swap_tp(value), axis)
        return lax.all_gather(value, "tp", axis=axis, tiled=True)

    full_tokens = gathered(tokens, 1).astype(jnp.float32)
    inverse_rms = lax.rsqrt(
        jnp.sum(full_tokens * full_tokens, axis=1) / model_width + eps_norm
    )
    scaled = (full_tokens * mix_gain).astype(jnp.bfloat16)
    latent_t = jnp.einsum(
        "kc,rk->cr",
        jnp.concatenate([w_kvlat, w_krope], axis=1),
        scaled,
        preferred_element_type=jnp.float32,
    )
    latent_t = (latent_t * inverse_rms[None, :]).astype(jnp.bfloat16)
    rotary_t = latent_t[latent_cols:].astype(jnp.float32)
    latent_t = latent_t[:latent_cols]
    projected = jnp.dot(
        scaled, jnp.concatenate([w_qlat, w_pool_in], axis=1), preferred_element_type=jnp.float32
    )
    projected = (projected * inverse_rms[:, None]).astype(jnp.bfloat16)
    query_part = projected[:, :query_cols]
    pool_pre = projected[:, query_cols:]

    positions = seq_rank * local_rows + jnp.arange(local_rows, dtype=jnp.int32)
    cosine, sine_table = tables(positions, ROPE)

    if pair:
        other_t = swap_tp(latent_t)
        pieces = [latent_t, other_t]
    else:
        pieces = [lax.all_gather(latent_t, "tp", axis=0, tiled=True)]
    squares = sum(
        jnp.sum(jnp.square(piece.astype(jnp.float32)), axis=0, keepdims=True) for piece in pieces
    )
    kv_inverse = lax.rsqrt(squares / (latent_cols * tp_size) + eps_norm)
    first_rot = rotary_t[:half] * cosine.T - rotary_t[half:] * sine_table.T
    second_rot = rotary_t[half:] * cosine.T + rotary_t[:half] * sine_table.T
    if pair:
        low, high = kv_gain[:latent_cols], kv_gain[latent_cols:]
        gains = [jnp.where(tp_rank == 0, low, high), jnp.where(tp_rank == 0, high, low)]
        rots = [
            jnp.where(tp_rank == 0, first_rot, second_rot),
            jnp.where(tp_rank == 0, second_rot, first_rot),
        ]
    else:
        gains = [kv_gain]
        rots = [jnp.concatenate([first_rot, second_rot], axis=0)]
    own_block = [
        jnp.concatenate([piece.astype(jnp.float32) * kv_inverse * gain[:, None], rot], axis=0).astype(
            jnp.bfloat16
        )
        for piece, gain, rot in zip(pieces, gains, rots)
    ]

    def sequence_pairs(keep):
        pairs = []
        for source in range(SPAN):
            for target in range(SPAN):
                if keep(source, target):
                    for seq in range(seq_count):
                        pairs.append((source * seq_count + seq, target * seq_count + seq))
        return pairs

    def with_other(value):
        if pair:
            return [value, swap_tp(value)]
        return [value]

    send = own_block[0]
    plane_pairs = lambda bits, causal: sequence_pairs(
        lambda s, t: t == s ^ bits and (t > s or not causal)
    )
    near = [shifted(send, "sp", plane_pairs(bits, True)) for bits in (1, 2, 3)]
    up = []
    for hop in range(1, SPAN // PLANE):
        moved = shifted(
            send if hop == 1 else up[-1][0],
            "sp",
            sequence_pairs(lambda s, t: t == s + PLANE and s >= PLANE * (hop - 1)),
        )
        up.append([moved])
    for row in up:
        row.extend(shifted(row[0], "sp", plane_pairs(bits, False)) for bits in (1, 2, 3))
    near = [with_other(value) for value in near]
    up = [[with_other(value) for value in row] for row in up]

    query_latent = gathered(query_part, 1).astype(jnp.float32)
    query_normed = (
        query_latent
        * lax.rsqrt(jnp.mean(query_latent * query_latent, axis=-1, keepdims=True) + eps_norm)
        * q_gain
    ).astype(jnp.bfloat16)
    query_content = (
        jnp.dot(query_normed, w_q_content, preferred_element_type=jnp.float32)
        .astype(jnp.bfloat16)
        .reshape(local_rows, own_heads, NOPE)
    )
    query_raw = jnp.dot(query_normed, w_q_rotary, preferred_element_type=jnp.float32).reshape(
        local_rows, own_heads, ROPE
    )
    cos_q, sin_q = cosine[:, None, :], sine_table[:, None, :]
    q_first = query_raw[..., :half] * cos_q - query_raw[..., half:] * sin_q
    q_second = query_raw[..., half:] * cos_q + query_raw[..., :half] * sin_q
    if pair:
        q_first, q_second = (
            jnp.where(tp_rank == 0, q_first, q_second),
            jnp.where(tp_rank == 0, q_second, q_first),
        )
    queries = jnp.concatenate(
        [query_content, q_first.astype(jnp.bfloat16), q_second.astype(jnp.bfloat16)], axis=-1
    ).transpose(1, 0, 2)

    def split_weight(weight):
        turned = weight.T
        if not pair:
            return [turned]
        low, high = turned[:, :latent_cols], turned[:, latent_cols:]
        return [jnp.where(tp_rank == 0, low, high), jnp.where(tp_rank == 0, high, low)]

    wk = split_weight(w_key)
    wv = split_weight(w_value)
    scale = (NOPE + ROPE) ** (-0.5)

    in_plane = seq_rank % PLANE
    plane = seq_rank // PLANE
    call = functools.partial(attn_call, queries=queries, wk=wk, wv=wv, scale=scale)
    no_flags = jnp.zeros((4,), jnp.int32)
    state = call(
        flags=no_flags, blocks=[own_block], groups=[[0]], state=None, last=False, diagonal=True
    )
    near_flags = jnp.stack([((in_plane ^ bits) < in_plane).astype(jnp.int32) for bits in (1, 2, 3)])
    state = call(
        flags=near_flags,
        blocks=near,
        groups=[[0], [1], [2]],
        state=state,
        last=False,
        diagonal=False,
    )
    for hop in range(1, SPAN // PLANE):
        state = call(
            flags=jnp.full((2,), (plane >= hop).astype(jnp.int32)),
            blocks=up[hop - 1],
            groups=[[0, 1], [2, 3]],
            state=state,
            last=hop == SPAN // PLANE - 1,
            diagonal=False,
        )
    attended, log_total = state

    group_count = pool_cols // GROUP_DIM
    rim_rows = shifted(
        pool_pre[local_rows - WIDEST :], "sp", sequence_pairs(lambda s, t: t == s + 1)
    )[1:]
    pool_values = pool_pre.astype(jnp.float32)
    extended = jnp.concatenate([rim_rows.astype(jnp.float32), pool_values], axis=0)
    groups = tp_rank * group_count + jnp.arange(pool_cols, dtype=jnp.int32) // GROUP_DIM
    windows = jnp.left_shift(jnp.int32(2), groups % 4)
    window_sums = jnp.zeros((local_rows, pool_cols), jnp.float32)
    for distance in range(WIDEST):
        window_sums = window_sums + jnp.where(
            distance < windows[None, :],
            extended[WIDEST - 1 - distance : WIDEST - 1 - distance + local_rows],
            0.0,
        )
    counts = jnp.minimum(positions[:, None] + 1, windows[None, :]).astype(jnp.float32)
    pooled = (window_sums / counts - pool_values).astype(jnp.bfloat16)
    own_mix = lax.dynamic_slice_in_dim(pool_mix, tp_rank * group_count, group_count, 0)
    mixed_pool = jnp.einsum(
        "rgc,gcd->rgd",
        pooled.reshape(local_rows, group_count, GROUP_DIM),
        own_mix,
        preferred_element_type=jnp.float32,
    ).reshape(local_rows, pool_cols)
    own_scale = lax.dynamic_slice_in_dim(pool_scale, tp_rank * pool_cols, pool_cols)
    pool_out = (mixed_pool * own_scale).astype(jnp.bfloat16)

    partial = jnp.dot(pool_out, w_out_pool, preferred_element_type=jnp.float32) + jnp.dot(
        attended, w_out_attn, preferred_element_type=jnp.float32
    )
    if pair:
        share = local_rows // 2
        kept = lax.dynamic_slice_in_dim(partial, tp_rank * share, share, 0)
        sent = lax.dynamic_slice_in_dim(partial, (1 - tp_rank) * share, share, 0)
        layer_out = (kept + swap_tp(sent.astype(jnp.bfloat16)).astype(jnp.float32)).astype(
            jnp.bfloat16
        )
    else:
        layer_out = lax.psum_scatter(
            partial.astype(jnp.bfloat16), "tp", scatter_dimension=0, tiled=True
        )
    return (layer_out, log_total)


def solution(mesh):
    in_specs = (
        P("sp", "tp"),
        P(),
        P(None, "tp"),
        P(None, "tp"),
        P(None, "tp"),
        P(),
        P(),
        P(),
        P(None, "tp"),
        P(None, "tp"),
        P(None, "tp"),
        P(None, "tp"),
        P(),
        P(),
        P("tp", None),
        P("tp", None),
    )
    out_specs = (P(("sp", "tp"), None), P("sp", "tp"))
    return jax.shard_map(
        per_device, mesh=mesh, in_specs=in_specs, out_specs=out_specs, check_vma=False
    )
```

```python
import functools

import jax
import jax.numpy as jnp
from jax import lax
from jax.experimental import pallas as pl
from jax.experimental.pallas import tpu as pltpu
from jax.sharding import PartitionSpec as P

NOPE = 128
ROPE = 64
VDIM = 128
GROUP_DIM = 128
WIDEST = 16
SPAN = 16
PLANE = 4
HALF = ROPE // 2

eps_norm = 1e-06
rope_base = 10000.0
masked_score = -1e30
log2e = 1.4426950408889634
score_scale = (NOPE + ROPE) ** (-0.5)


f32, bf16 = jnp.float32, jnp.bfloat16
vmem_spec = pl.BlockSpec(memory_space=pltpu.VMEM)
smem_spec = pl.BlockSpec(memory_space=pltpu.SMEM)
any_spec = pl.BlockSpec(memory_space=pl.ANY)
hbm_spec = pl.BlockSpec(memory_space=pltpu.HBM)


def dot(left, right):
    return jnp.dot(left, right, preferred_element_type=f32)


def slot_of(info, part, parts):
    if parts == 1:
        return 0
    return info[0] if part == 0 else 1 - info[0]


def simple_call(body, name, out_shape, operands, flops, specs=None, scratch=(), room=40):
    specs = specs or [smem_spec] + [vmem_spec] * (len(operands) - 1)
    return pl.pallas_call(
        body,
        name=name,
        out_shape=out_shape,
        in_specs=specs,
        out_specs=[vmem_spec] * len(out_shape),
        scratch_shapes=list(scratch),
        compiler_params=pltpu.CompilerParams(vmem_limit_bytes=room * 1024 * 1024),
        cost_estimate=pl.CostEstimate(
            flops=flops, bytes_accessed=8 * 1024 * 1024, transcendentals=0
        ),
    )(*operands)


def turn_body(info, key_ref, value_ref, key_out, value_out):
    parts, channels, _ = key_ref.shape
    for source, target in ((key_ref, key_out), (value_ref, value_out)):
        for part in range(parts):
            turned = source[slot_of(info, part, parts)].T
            target[:, part * channels : (part + 1) * channels] = turned


def project_body(info, *refs, parts):
    tokens = refs[:parts]
    gain = refs[parts]
    weights_hbm = refs[parts + 1 : parts + 5]
    kv_out, rope_out, query_out, pool_out = refs[parts + 5 : parts + 9]
    weights, sems = refs[parts + 9 : parts + 13], refs[parts + 13]
    copies = [
        pltpu.make_async_copy(weights_hbm[index], weights[index], sems.at[index])
        for index in range(4)
    ]
    for copy in copies:
        copy.start()
    squares = None
    scaled = []
    for part in range(parts):
        values = tokens[part][...].astype(f32)
        square = jnp.sum(values * values, axis=1, keepdims=True)
        squares = square if squares is None else squares + square
        scaled.append((values * gain[slot_of(info, part, parts)]).astype(bf16))
    width = parts * tokens[0].shape[1]
    inverse = lax.rsqrt(squares / width + eps_norm)

    def product(index):
        copies[index].wait()
        total = None
        for part in range(parts):
            depth = scaled[part].shape[1]
            start = pl.multiple_of(slot_of(info, part, parts) * depth, depth)
            if index == 1:
                piece = lax.dot_general(
                    scaled[part],
                    weights[index][:, pl.ds(start, depth)],
                    (((1,), (1,)), ((), ())),
                    preferred_element_type=f32,
                )
            else:
                piece = dot(scaled[part], weights[index][pl.ds(start, depth), :])
            total = piece if total is None else total + piece
        return (total * inverse).astype(bf16)

    kv_out[...] = product(0).T
    rope = product(1).astype(f32)
    rope_out[...] = jnp.concatenate([rope, jnp.zeros_like(rope)], axis=1).T[:ROPE]
    query_out[...] = product(2)
    pool_out[...] = product(3)


def key_body(info, *refs, parts):
    latents = refs[:parts]
    rope, gain, cosine, sine = refs[parts : parts + 4]
    blocks = refs[parts + 4 :]
    values = [latent[...].astype(f32) for latent in latents]
    squares = sum(jnp.sum(value * value, axis=0, keepdims=True) for value in values)
    channels = values[0].shape[0]
    inverse = lax.rsqrt(squares / (channels * parts) + eps_norm)
    first = rope[:HALF] * cosine[...] - rope[HALF:] * sine[...]
    second = rope[HALF:] * cosine[...] + rope[:HALF] * sine[...]
    for part in range(parts):
        slot = slot_of(info, part, parts)
        blocks[part][:channels] = (values[part] * inverse * gain[slot]).astype(bf16)
        if parts == 1:
            blocks[part][channels : channels + HALF] = first.astype(bf16)
            blocks[part][channels + HALF :] = second.astype(bf16)
        else:
            blocks[part][channels:] = jnp.where(slot == 0, first, second).astype(bf16)


def query_body(info, *refs, parts, heads):
    latents = refs[:parts]
    gain, w_content, w_rotary, cosine, sine, out = refs[parts:]
    values = [latent[...].astype(f32) for latent in latents]
    squares = sum(jnp.sum(value * value, axis=1, keepdims=True) for value in values)
    inverse = lax.rsqrt(squares / (values[0].shape[1] * parts) + eps_norm)
    content = rotary = None
    for part in range(parts):
        slot = slot_of(info, part, parts)
        normed = (values[part] * inverse * gain[slot]).astype(bf16)
        content_part = dot(normed, w_content[slot])
        rotary_part = dot(normed, w_rotary[slot])
        content = content_part if content is None else content + content_part
        rotary = rotary_part if rotary is None else rotary + rotary_part
    lane = lax.broadcasted_iota(jnp.int32, (values[0].shape[0], 128), 1)
    low_half = lane % ROPE < HALF
    for head in range(0, heads, 2):
        raw = rotary[:, head * ROPE : head * ROPE + 128]
        swapped = jnp.where(low_half, pltpu.roll(raw, 128 - HALF, 1), pltpu.roll(raw, HALF, 1))
        turned = raw * cosine[...] + swapped * sine[...]
        out[head, :, NOPE:] = turned[:, :ROPE].astype(bf16)
        out[head + 1, :, NOPE:] = pltpu.roll(turned, ROPE, 1)[:, :ROPE].astype(bf16)
    for head in range(heads):
        out[head, :, :NOPE] = content[:, head * NOPE : (head + 1) * NOPE].astype(bf16)


def stack_body(left, right, out):
    out[0], out[1] = left[...], right[...]


def stack_pair(left, right):
    return pl.pallas_call(
        stack_body,
        name="stack_pair",
        out_shape=jax.ShapeDtypeStruct((2,) + left.shape, left.dtype),
        in_specs=[vmem_spec] * 2,
        out_specs=vmem_spec,
        compiler_params=pltpu.CompilerParams(vmem_limit_bytes=8 * 1024 * 1024),
    )(left, right)


def pool_body(info, pool_ref, rim_ref, mix_ref, scale_ref, out_ref):
    rows, cols = pool_ref.shape
    count = cols // GROUP_DIM
    place = lax.broadcasted_iota(jnp.int32, (rows, GROUP_DIM), 0) + info[1] * rows + 1
    for index in range(count):
        span = slice(index * GROUP_DIM, (index + 1) * GROUP_DIM)
        group = info[0] * count + index
        own = pool_ref[:, span].astype(f32)
        total = jnp.concatenate([rim_ref[:, span].astype(f32), own], axis=0)
        stages = []
        for step in (1, 2, 4, 8):
            total = total + pltpu.roll(total, step, 0)
            stages.append(total[WIDEST:])
        if count % 4 == 0:
            window = 2 << (index % 4)
            sums = stages[index % 4]
        else:
            window = jnp.left_shift(jnp.int32(2), group % 4)
            sums = stages[3]
            for stage in range(3):
                sums = jnp.where(group % 4 == stage, stages[stage], sums)
        pooled = sums / jnp.minimum(place, window).astype(f32) - own
        mixed = dot(pooled.astype(bf16), mix_ref[group])
        out_ref[:, span] = (mixed * scale_ref[group]).astype(bf16)


def attn_body(*refs, arrays, group, parts, heads, first, last, diagonal, masked, flags):
    refs = list(refs)
    take = lambda count: [refs.pop(0) for _ in range(count)]
    info, q_ref, wk_ref, wv_ref = take(4)
    blocks = []
    for _ in range(arrays):
        array = take(parts)
        if len(array[0].shape) == 2:
            blocks.append(array)
        else:
            blocks.extend([ref.at[at] for ref in array] for at in range(array[0].shape[0]))
    state_in = take(4)[:3] if not first else None
    if last:
        pool_ref, w_pool_hbm, w_attn_hbm = take(3)
        outs = take(2 if parts == 2 else 1)
        log_ref = refs.pop(0)
        state = take(3)
    else:
        state = take(3)
        tie_ref = refs.pop(0)
    kt_ref, vt_ref = take(2)
    max_ref, sum_ref, acc_ref = state
    keys = blocks[0][0].shape[-1]
    factor = score_scale * log2e
    if last:
        w_pool_ref, w_attn_ref, attended_ref, sems = take(4)
        copies = [
            pltpu.make_async_copy(w_attn_hbm, w_attn_ref, sems.at[0]),
            pltpu.make_async_copy(w_pool_hbm, w_pool_ref, sems.at[1]),
        ]
        for copy in copies:
            copy.start()

    count = len(blocks) // group
    width = group * keys

    def project(block, into, at):
        span = slice(at * keys, (at + 1) * keys)
        channels = wk_ref.shape[1] // parts
        k_rows = v_rows = None
        for part in range(parts):
            piece = block[part][:channels, :]
            cols = slice(part * channels, (part + 1) * channels)
            k_part, v_part = dot(wk_ref[:, cols], piece), dot(wv_ref[:, cols], piece)
            k_rows = k_part if k_rows is None else k_rows + k_part
            v_rows = v_part if v_rows is None else v_rows + v_part
        k_rows = k_rows.astype(bf16)
        vt_ref[into, :, span] = v_rows.astype(bf16)
        turn = ROPE // parts
        for head in range(heads):
            kt_ref[into, head, :NOPE, span] = k_rows[head * NOPE : (head + 1) * NOPE]
            for part in range(parts):
                low = pl.multiple_of(NOPE + slot_of(info, part, parts) * turn, turn)
                kt_ref[into, head, pl.ds(low, turn), span] = block[part][channels:, :]

    def scores_of(into, head):
        return dot(q_ref[head], kt_ref[into, head])

    def absorb(into, head, scores, source):
        tiles = [scores[:, tile * 128 : (tile + 1) * 128] for tile in range(width // 128)]
        if diagonal:
            row = lax.broadcasted_iota(jnp.int32, tiles[0].shape, 0)
            col = lax.broadcasted_iota(jnp.int32, tiles[0].shape, 1)
            tiles = [
                jnp.where(col + tile * 128 <= row, value, masked_score)
                for tile, value in enumerate(tiles)
            ]
        elif masked and group > 1:
            bias = [jnp.where(flag_of(into, at) != 0, 0.0, masked_score) for at in range(group)]
            tiles = [value + bias[tile * 128 // keys] for tile, value in enumerate(tiles)]
        peak = functools.reduce(jnp.maximum, tiles)
        peak = jnp.max(peak, axis=1, keepdims=True)
        if source is None:
            new = jnp.broadcast_to(peak, tiles[0].shape)
            total = None
        else:
            old = source[0][head]
            new = jnp.maximum(old, peak)
            shrink = jnp.exp2((old - new) * factor)
            total = source[1][head] * shrink
        weights = []
        for value in tiles:
            expo = jnp.exp2((value - new) * factor)
            total = expo if total is None else total + expo
            weights.append(expo.astype(bf16))
        update = lax.dot_general(
            jnp.concatenate(weights, axis=1),
            vt_ref[into, head * VDIM : (head + 1) * VDIM, :],
            (((1,), (1,)), ((), ())),
            preferred_element_type=f32,
        )
        max_ref[head] = new
        sum_ref[head] = total
        acc_ref[head] = update if source is None else source[2][head] * shrink + update

    def flag_of(into, at):
        if isinstance(into, int):
            return info[flags[into * group + at]]
        values = [info[flags[index * group + at]] for index in range(count)]
        return functools.reduce(
            lambda rest, index: jnp.where(into == index, values[index], rest),
            range(1, count),
            values[0],
        )

    def soften(into, source):
        scores = scores_of(into, 0)
        for head in range(heads):
            ahead = scores_of(into, head + 1) if head + 1 < heads else None
            absorb(into, head, scores, source)
            scores = ahead

    def keep_state():
        for kept, target in zip(state_in, state):
            target[...] = kept[...]

    def enter(into):
        for at in range(group):
            project(blocks[into * group + at], into, at)

    def wanted(into):
        flag = flag_of(into, 0)
        for at in range(1, group):
            flag = flag | flag_of(into, at)
        return flag

    if first:
        enter(0)
        soften(0, None)
    elif count == 1:

        @pl.when(wanted(0) != 0)
        def _():
            enter(0)
            soften(0, state_in)

        pl.when(wanted(0) == 0)(keep_state)
    else:
        keep_state()
        for into in range(count):
            pl.when(wanted(into) != 0)(functools.partial(enter, into))

        def turn(into, carry):
            pl.when(wanted(into) != 0)(lambda: soften(into, state))
            return carry

        lax.fori_loop(0, count, turn, 0)

    if not last:
        tie_ref[...] = sum_ref[0, :8]
    if last:
        lane = lax.broadcasted_iota(jnp.int32, (q_ref.shape[1], 128), 1)
        for head in range(heads):
            total = jnp.sum(sum_ref[head], axis=1, keepdims=True)
            attended_ref[:, head * VDIM : (head + 1) * VDIM] = (acc_ref[head] / total).astype(bf16)
            column = max_ref[head] * score_scale + jnp.log(total)
            logs = column if head == 0 else jnp.where(lane == head, column, logs)
        log_ref[...] = logs.T[:heads]
        for copy in copies:
            copy.wait()
        rows = attended_ref.shape[0] // len(outs)
        for index, out in enumerate(outs):
            start = 0
            if len(outs) == 2:
                start = pl.multiple_of((info[0] if index == 0 else 1 - info[0]) * rows, rows)
            result = dot(attended_ref[pl.ds(start, rows), :], w_attn_ref[...])
            result = result + dot(pool_ref[pl.ds(start, rows), :], w_pool_ref[...])
            out[...] = result.astype(out.dtype)


def attn_call(name, info, queries, wk, wv, blocks, group, state, flags, diagonal=False, masked=False, tail=None):
    heads, rows, _ = queries.shape
    first, last = state is None, tail is not None
    parts = len(blocks[0])
    keys = blocks[0][0].shape[-1]
    width = group * keys
    total = sum(1 if block[0].ndim == 2 else block[0].shape[0] for block in blocks)
    count = total // group
    body = functools.partial(
        attn_body,
        arrays=len(blocks),
        group=group,
        parts=parts,
        heads=heads,
        first=first,
        last=last,
        diagonal=diagonal,
        masked=masked,
        flags=flags,
    )
    operands = [info, queries, wk, wv]
    for block in blocks:
        operands.extend(block)
    specs = [smem_spec] + [vmem_spec] * (len(operands) - 1)
    state_shape = jax.ShapeDtypeStruct((heads, rows, 128), f32)
    aliases = {}
    if not first:
        if not last:
            aliases = {len(operands) + i: i for i in range(3)}
        operands.extend(state)
        specs.extend([vmem_spec] * 3 + [any_spec])
    scratch = [
        pltpu.VMEM((count, heads, NOPE + ROPE, width), bf16),
        pltpu.VMEM((count, heads * VDIM, width), bf16),
    ]
    flops = total * keys * heads * 2
    flops = flops * (rows * (NOPE + ROPE + VDIM) + (NOPE + VDIM) * wk.shape[1])
    if last:
        pool_out, w_pool, w_attn = tail
        operands.extend(tail)
        specs.extend([vmem_spec, hbm_spec, hbm_spec])
        model = w_pool.shape[1]
        if parts == 2:
            out_shape = [
                jax.ShapeDtypeStruct((rows // 2, model), f32),
                jax.ShapeDtypeStruct((rows // 2, model), bf16),
            ]
        else:
            out_shape = [jax.ShapeDtypeStruct((rows, model), bf16)]
        out_shape.append(jax.ShapeDtypeStruct((heads, rows), f32))
        scratch = [pltpu.VMEM(state_shape.shape, f32)] * 3 + scratch
        scratch += [
            pltpu.VMEM(w_pool.shape, bf16),
            pltpu.VMEM(w_attn.shape, bf16),
            pltpu.VMEM((rows, heads * VDIM), bf16),
            pltpu.SemaphoreType.DMA((2,)),
        ]
    else:
        out_shape = [state_shape] * 3 + [jax.ShapeDtypeStruct((8, 128), f32)]
    results = pl.pallas_call(
        body,
        name=name,
        out_shape=out_shape,
        in_specs=specs,
        out_specs=[vmem_spec] * len(out_shape),
        scratch_shapes=scratch,
        input_output_aliases=aliases,
        compiler_params=pltpu.CompilerParams(vmem_limit_bytes=40 * 1024 * 1024),
        cost_estimate=pl.CostEstimate(
            flops=flops, bytes_accessed=20 * 1024 * 1024, transcendentals=flops // 600
        ),
    )(*operands)
    return results if last else (results[:3], results[3])


def per_device(
    tokens,
    mix_gain,
    w_pool_in,
    w_qlat,
    w_kvlat,
    w_krope,
    q_gain,
    kv_gain,
    w_q_content,
    w_q_rotary,
    w_key,
    w_value,
    pool_mix,
    pool_scale,
    w_out_pool,
    w_out_attn,
):
    tp_size = lax.axis_size("tp")
    tp_rank = lax.axis_index("tp")
    seq_count = lax.axis_size("sp") // SPAN
    seq_rank = lax.axis_index("sp") // seq_count
    rows, own_width = tokens.shape
    model_width = own_width * tp_size
    pool_cols = w_pool_in.shape[1]
    query_cols = w_qlat.shape[1]
    kv_cols = w_kvlat.shape[1]
    heads = w_key.shape[1] // NOPE
    parts = 2 if tp_size == 2 else 1
    in_plane, plane = seq_rank % PLANE, seq_rank // PLANE

    def swapped(value):
        return lax.ppermute(value, "tp", [(0, 1), (1, 0)])

    def both(value, axis):
        if parts == 2:
            return [value, swapped(value)]
        return [lax.all_gather(value, "tp", axis=axis, tiled=True)]

    def moved(value, keep):
        pairs = [
            (source * seq_count + seq, target * seq_count + seq)
            for source in range(SPAN)
            for target in range(SPAN)
            if keep(source, target)
            for seq in range(seq_count)
        ]
        return lax.ppermute(value, "sp", pairs)

    def by_part(value):
        return value.reshape((parts, value.shape[0] // parts) + value.shape[1:])

    info = jnp.stack(
        [tp_rank, seq_rank, in_plane % 2, in_plane // 2]
        + [(plane >= hop).astype(jnp.int32) for hop in range(1, SPAN // PLANE)]
    ).astype(jnp.int32)
    positions = (seq_rank * rows + jnp.arange(rows, dtype=jnp.int32)).astype(f32)
    frequency = rope_base ** (-jnp.arange(HALF, dtype=f32) * 2.0 / ROPE)
    angles = frequency[:, None] * positions[None, :]
    cosine, sine = jnp.cos(angles), jnp.sin(angles)
    lane = jnp.arange(128, dtype=jnp.int32)
    lane_frequency = rope_base ** (-(lane % HALF).astype(f32) * 2.0 / ROPE)
    lane_angles = positions[:, None] * lane_frequency[None, :]
    lane_cos = jnp.cos(lane_angles)
    lane_sin = jnp.where(lane % ROPE < HALF, -1.0, 1.0)[None, :] * jnp.sin(lane_angles)

    token_parts = both(tokens, 1)
    *token_parts, cosine, sine, lane_cos, lane_sin, info = lax.optimization_barrier(
        (*token_parts, cosine, sine, lane_cos, lane_sin, info)
    )
    in_weights = [w_kvlat, w_krope.T, w_qlat, w_pool_in]
    kv_part, rope_t, query_part, pool_pre = simple_call(
        functools.partial(project_body, parts=parts),
        "project",
        [
            jax.ShapeDtypeStruct((kv_cols, rows), bf16),
            jax.ShapeDtypeStruct((ROPE, rows), f32),
            jax.ShapeDtypeStruct((rows, query_cols), bf16),
            jax.ShapeDtypeStruct((rows, pool_cols), bf16),
        ],
        [info, *token_parts, mix_gain.reshape(parts, 1, model_width // parts), *in_weights],
        2 * 10**9,
        specs=[smem_spec] + [vmem_spec] * (parts + 1) + [hbm_spec] * 4,
        scratch=[pltpu.VMEM(weight.shape, bf16) for weight in in_weights]
        + [pltpu.SemaphoreType.DMA((4,))],
        room=60,
    )
    kv_parts = both(kv_part, 0)
    rim = moved(pool_pre[rows - WIDEST :], lambda s, t: t == s + 1)
    query_parts = both(query_part, 1)
    latent = kv_parts[0].shape[0] * parts
    own_block = simple_call(
        functools.partial(key_body, parts=parts),
        "keys",
        [jax.ShapeDtypeStruct(((latent + ROPE) // parts, rows), bf16)] * parts,
        [info, *kv_parts, rope_t, by_part(kv_gain[:, None]), cosine, sine],
        10**8,
    )

    send = own_block[0]
    x_of = lambda s, t: t == s ^ 1
    y_of = lambda s, t: t == s ^ 2
    rising = lambda rule: lambda s, t: t > s and rule(s, t)
    def with_other(value):
        return [value, swapped(value)] if parts == 2 else [value]

    def step_up(value, hop):
        return moved(value, lambda s, t: t == s + PLANE and s >= PLANE * (hop - 1))

    def within(value, rule, hop):
        return moved(value, lambda s, t: s >= PLANE * hop and rule(s, t))

    hold = lax.optimization_barrier
    near_x, near_y, up1 = moved(send, x_of), moved(send, rising(y_of)), step_up(send, 1)

    wk, wv = simple_call(
        turn_body,
        "turn_weights",
        [jax.ShapeDtypeStruct((weight.shape[1], weight.shape[0]), bf16) for weight in (w_key, w_value)],
        [info, by_part(w_key), by_part(w_value)],
        2 * 10**8,
    )
    queries = simple_call(
        functools.partial(query_body, parts=parts, heads=heads),
        "queries",
        [jax.ShapeDtypeStruct((heads, rows, NOPE + ROPE), bf16)],
        [
            info,
            *query_parts,
            q_gain.reshape(parts, 1, q_gain.shape[0] // parts),
            by_part(w_q_content),
            by_part(w_q_rotary),
            lane_cos,
            lane_sin,
        ],
        6 * 10**8,
    )[0]
    def attend(name, state, blocks, flags, group=2, **options):
        return attn_call(name, info, queries, wk, wv, blocks, group, state, flags, **options)

    flag_x, flag_y, *above = range(2, 3 + SPAN // PLANE)
    above = [None] + above
    state, tie = attend("own", None, [own_block], (), 1, diagonal=True)
    tie, near_x, near_y, up1 = hold((tie, near_x, near_y, up1))
    near = [with_other(near_x), with_other(near_y)]
    far, beside1, up2 = moved(near_x, rising(y_of)), within(up1, x_of, 1), step_up(up1, 2)
    state, tie = attend("near", (*state, tie), near, (flag_x, flag_y), masked=True)
    tie, far, up1, beside1, up2, rim = hold((tie, far, up1, beside1, up2, rim))
    ready = [with_other(value) for value in (far, up1, beside1)]
    across = within(stack_pair(up1, up2), y_of, 1)
    beside2, up3 = within(up2, x_of, 2), step_up(up2, 3)
    pool_out = simple_call(
        pool_body,
        "pool",
        [jax.ShapeDtypeStruct((rows, pool_cols), bf16)],
        [
            info,
            pool_pre,
            rim,
            pool_mix,
            pool_scale.reshape(pool_scale.shape[0] // GROUP_DIM, 1, GROUP_DIM),
        ],
        10**8,
    )[0]
    state, tie = attend("up1", (*state, tie), ready, (flag_y, above[1], above[1]), 3, masked=True)
    tie, up2, beside2, across, up3 = hold((tie, up2, beside2, across, up3))
    ready = [with_other(value) for value in (up2, beside2, across)]
    corner, across3 = within(across, x_of, 1), within(up3, y_of, 3)
    state, tie = attend("up2", (*state, tie), ready, (above[2], above[2], above[1], above[2]), masked=True)
    tie, corner, up3, across3 = hold((tie, corner, up3, across3))
    ready = [with_other(value) for value in (corner, up3, across3)]
    last = within(stack_pair(up3, across3), x_of, 3)
    state, tie = attend("up3", (*state, tie), ready, (above[1], above[2], above[3], above[3]), masked=True)
    tie, last = hold((tie, last))
    state = attend(
        "end",
        (*state, tie),
        [with_other(last)],
        (above[3], above[3]),
        tail=(pool_out, w_out_pool, w_out_attn),
    )
    if parts == 2:
        kept, sent, log_total = state
        layer_out = (kept + swapped(sent).astype(f32)).astype(bf16)
    else:
        partial, log_total = state
        layer_out = lax.psum_scatter(partial, "tp", scatter_dimension=0, tiled=True)
    return (layer_out, log_total.T)


def solution(mesh):
    split = P(None, "tp")
    in_specs = (
        P("sp", "tp"),
        P(),
        split,
        split,
        split,
        P(),
        P(),
        P(),
        split,
        split,
        split,
        split,
        P(),
        P(),
        P("tp", None),
        P("tp", None),
    )
    out_specs = (P(("sp", "tp"), None), P("sp", "tp"))
    return jax.shard_map(
        per_device, mesh=mesh, in_specs=in_specs, out_specs=out_specs, check_vma=False
    )
```

```python
import functools

import jax
import jax.numpy as jnp
from jax import lax
from jax.experimental import pallas as pl
from jax.experimental.pallas import tpu as pltpu
from jax.sharding import PartitionSpec as P

NOPE = 128
ROPE = 64
VDIM = 128
GROUP_DIM = 128
WIDEST = 16
SPAN = 16
PLANE = 4
HALF = ROPE // 2

eps_norm = 1e-06
rope_base = 10000.0
masked_score = -1e30
log2e = 1.4426950408889634
score_scale = (NOPE + ROPE) ** (-0.5)


f32, bf16 = jnp.float32, jnp.bfloat16
vmem_spec = pl.BlockSpec(memory_space=pltpu.VMEM)
smem_spec = pl.BlockSpec(memory_space=pltpu.SMEM)
any_spec = pl.BlockSpec(memory_space=pl.ANY)
hbm_spec = pl.BlockSpec(memory_space=pltpu.HBM)


def dot(left, right):
    return jnp.dot(left, right, preferred_element_type=f32)


def slot_of(info, part, parts):
    if parts == 1:
        return 0
    return info[0] if part == 0 else 1 - info[0]


def simple_call(body, name, out_shape, operands, flops, specs=None, scratch=(), room=40):
    specs = specs or [smem_spec] + [vmem_spec] * (len(operands) - 1)
    return pl.pallas_call(
        body,
        name=name,
        out_shape=out_shape,
        in_specs=specs,
        out_specs=[vmem_spec] * len(out_shape),
        scratch_shapes=list(scratch),
        compiler_params=pltpu.CompilerParams(vmem_limit_bytes=room * 1024 * 1024),
        cost_estimate=pl.CostEstimate(
            flops=flops, bytes_accessed=8 * 1024 * 1024, transcendentals=0
        ),
    )(*operands)


def turn_body(info, key_ref, value_ref, key_out, value_out):
    parts, channels, _ = key_ref.shape
    for source, target in ((key_ref, key_out), (value_ref, value_out)):
        for part in range(parts):
            turned = source[slot_of(info, part, parts)].T
            target[:, part * channels : (part + 1) * channels] = turned


def project_body(info, *refs, parts):
    tokens = refs[:parts]
    gain, *weights = refs[parts : parts + 5]
    kv_out, rope_out, query_out, pool_out = refs[parts + 5 :]
    squares = None
    scaled = []
    for part in range(parts):
        values = tokens[part][...].astype(f32)
        square = jnp.sum(values * values, axis=1, keepdims=True)
        squares = square if squares is None else squares + square
        scaled.append((values * gain[slot_of(info, part, parts)]).astype(bf16))
    depth = tokens[0].shape[1]
    inverse = lax.rsqrt(squares / (depth * parts) + eps_norm)

    def product(index):
        total = None
        for part in range(parts):
            start = pl.multiple_of(slot_of(info, part, parts) * depth, depth)
            if index == 1:
                piece = lax.dot_general(
                    scaled[part],
                    weights[index][:, pl.ds(start, depth)],
                    (((1,), (1,)), ((), ())),
                    preferred_element_type=f32,
                )
            else:
                piece = dot(scaled[part], weights[index][pl.ds(start, depth), :])
            total = piece if total is None else total + piece
        return (total * inverse).astype(bf16)

    kv_out[...] = product(0).T
    rope = product(1).astype(f32)
    rope_out[...] = jnp.concatenate([rope, jnp.zeros_like(rope)], axis=1).T[:ROPE]
    query_out[...] = product(2)
    pool_out[...] = product(3)


def key_body(info, *refs, parts):
    latents = refs[:parts]
    rope, gain, cosine, sine = refs[parts : parts + 4]
    blocks = refs[parts + 4 :]
    values = [latent[...].astype(f32) for latent in latents]
    squares = sum(jnp.sum(value * value, axis=0, keepdims=True) for value in values)
    channels = values[0].shape[0]
    inverse = lax.rsqrt(squares / (channels * parts) + eps_norm)
    first = rope[:HALF] * cosine[...] - rope[HALF:] * sine[...]
    second = rope[HALF:] * cosine[...] + rope[:HALF] * sine[...]
    for part in range(parts):
        slot = slot_of(info, part, parts)
        blocks[part][:channels] = (values[part] * inverse * gain[slot]).astype(bf16)
        if parts == 1:
            blocks[part][channels : channels + HALF] = first.astype(bf16)
            blocks[part][channels + HALF :] = second.astype(bf16)
        else:
            blocks[part][channels:] = jnp.where(slot == 0, first, second).astype(bf16)


def query_body(info, *refs, parts, heads):
    latents = refs[:parts]
    gain, w_content, w_rotary, cosine, sine, out = refs[parts:]
    values = [latent[...].astype(f32) for latent in latents]
    squares = sum(jnp.sum(value * value, axis=1, keepdims=True) for value in values)
    inverse = lax.rsqrt(squares / (values[0].shape[1] * parts) + eps_norm)
    content = rotary = None
    for part in range(parts):
        slot = slot_of(info, part, parts)
        normed = (values[part] * inverse * gain[slot]).astype(bf16)
        content_part = dot(normed, w_content[slot])
        rotary_part = dot(normed, w_rotary[slot])
        content = content_part if content is None else content + content_part
        rotary = rotary_part if rotary is None else rotary + rotary_part
    lane = lax.broadcasted_iota(jnp.int32, (values[0].shape[0], 128), 1)
    low_half = lane % ROPE < HALF
    for head in range(0, heads, 2):
        raw = rotary[:, head * ROPE : head * ROPE + 128]
        swapped = jnp.where(low_half, pltpu.roll(raw, 128 - HALF, 1), pltpu.roll(raw, HALF, 1))
        turned = raw * cosine[...] + swapped * sine[...]
        out[head, :, NOPE:] = turned[:, :ROPE].astype(bf16)
        out[head + 1, :, NOPE:] = pltpu.roll(turned, ROPE, 1)[:, :ROPE].astype(bf16)
    for head in range(heads):
        out[head, :, :NOPE] = content[:, head * NOPE : (head + 1) * NOPE].astype(bf16)


def stack_body(left, right, out):
    out[0], out[1] = left[...], right[...]


def stack_pair(left, right):
    return pl.pallas_call(
        stack_body,
        name="stack_pair",
        out_shape=jax.ShapeDtypeStruct((2,) + left.shape, left.dtype),
        in_specs=[vmem_spec] * 2,
        out_specs=vmem_spec,
        compiler_params=pltpu.CompilerParams(vmem_limit_bytes=8 * 1024 * 1024),
    )(left, right)


def pool_body(info, pool_ref, rim_ref, mix_ref, scale_ref, out_ref):
    rows, cols = pool_ref.shape
    count = cols // GROUP_DIM
    place = lax.broadcasted_iota(jnp.int32, (rows, GROUP_DIM), 0) + info[1] * rows + 1
    for index in range(count):
        span = slice(index * GROUP_DIM, (index + 1) * GROUP_DIM)
        group = info[0] * count + index
        own = pool_ref[:, span].astype(f32)
        total = jnp.concatenate([rim_ref[:, span].astype(f32), own], axis=0)
        stages = []
        for step in (1, 2, 4, 8):
            total = total + pltpu.roll(total, step, 0)
            stages.append(total[WIDEST:])
        if count % 4 == 0:
            window = 2 << (index % 4)
            sums = stages[index % 4]
        else:
            window = jnp.left_shift(jnp.int32(2), group % 4)
            sums = stages[3]
            for stage in range(3):
                sums = jnp.where(group % 4 == stage, stages[stage], sums)
        pooled = sums / jnp.minimum(place, window).astype(f32) - own
        mixed = dot(pooled.astype(bf16), mix_ref[group])
        out_ref[:, span] = (mixed * scale_ref[group]).astype(bf16)


def attn_body(*refs, arrays, group, parts, heads, first, last, diagonal, masked, flags, halves):
    refs = list(refs)
    take = lambda count: [refs.pop(0) for _ in range(count)]
    info, q_ref, wk_ref, wv_ref = take(4)
    blocks = []
    for _ in range(arrays):
        array = take(parts)
        if len(array[0].shape) == 2:
            blocks.append(array)
        else:
            blocks.extend([ref.at[at] for ref in array] for at in range(array[0].shape[0]))
    state_in = take(4)[:3] if not first else None
    if last:
        pool_ref, w_pool_hbm, w_attn_hbm = take(3)
        outs = take(2 if parts == 2 else 1)
        log_ref = refs.pop(0)
        state = take(3)
    else:
        state = take(3)
        tie_ref = refs.pop(0)
    kt_ref, vt_ref, lat_ref = take(3)
    max_ref, sum_ref, acc_ref = state
    keys = blocks[0][0].shape[-1]
    factor = score_scale * log2e
    if last:
        w_pool_ref, w_attn_ref, attended_ref, sems = take(4)
        copies = [
            pltpu.make_async_copy(w_attn_hbm, w_attn_ref, sems.at[0]),
            pltpu.make_async_copy(w_pool_hbm, w_pool_ref, sems.at[1]),
        ]
        for copy in copies:
            copy.start()

    count = len(blocks) // group
    width = group * keys

    def lay(block, at):
        channels = block[0].shape[0] - ROPE // parts
        for part in range(parts):
            lat_ref[at, part * channels : (part + 1) * channels] = block[part][:channels, :]
            turn = ROPE // parts
            low = parts * channels + slot_of(info, part, parts) * turn
            lat_ref[at, pl.ds(pl.multiple_of(low, turn), turn)] = block[part][channels:, :]

    def project(at):
        into, place = lax.div(at, group), lax.rem(at, group)
        span = pl.ds(pl.multiple_of(place * keys, 128), keys)
        latent = wk_ref.shape[1]
        k_rows = dot(wk_ref[...], lat_ref[at, :latent]).astype(bf16)
        vt_ref[into, :, span] = dot(wv_ref[...], lat_ref[at, :latent]).astype(bf16)
        for head in range(heads):
            kt_ref[into, head, :NOPE, span] = k_rows[head * NOPE : (head + 1) * NOPE]
            kt_ref[into, head, NOPE:, span] = lat_ref[at, latent:]

    def scores_of(into, head):
        return dot(q_ref[head], kt_ref[into, head])

    def absorb(into, head, scores, source):
        tiles = [scores[:, tile * 128 : (tile + 1) * 128] for tile in range(width // 128)]
        if diagonal:
            row = lax.broadcasted_iota(jnp.int32, tiles[0].shape, 0)
            col = lax.broadcasted_iota(jnp.int32, tiles[0].shape, 1)
            tiles = [
                jnp.where(col + tile * 128 <= row, value, masked_score)
                for tile, value in enumerate(tiles)
            ]
        elif masked and group > 1:
            bias = [jnp.where(flag_of(into, at) != 0, 0.0, masked_score) for at in range(group)]
            tiles = [value + bias[tile * 128 // keys] for tile, value in enumerate(tiles)]
        peak = functools.reduce(jnp.maximum, tiles)
        peak = jnp.max(peak, axis=1, keepdims=True)
        if source is None:
            new = jnp.broadcast_to(peak, tiles[0].shape)
            total = None
        else:
            old = source[0][head]
            new = jnp.maximum(old, peak)
            shrink = jnp.exp2((old - new) * factor)
            total = source[1][head] * shrink
        weights = []
        for value in tiles:
            expo = jnp.exp2((value - new) * factor)
            total = expo if total is None else total + expo
            weights.append(expo.astype(bf16))
        update = lax.dot_general(
            jnp.concatenate(weights, axis=1),
            vt_ref[into, pl.ds(pl.multiple_of(head * VDIM, VDIM), VDIM), :],
            (((1,), (1,)), ((), ())),
            preferred_element_type=f32,
        )
        max_ref[head] = new
        sum_ref[head] = total
        acc_ref[head] = update if source is None else source[2][head] * shrink + update

    def flag_of(into, at):
        if isinstance(into, int):
            return info[flags[into * group + at]]
        values = [info[flags[index * group + at]] for index in range(count)]
        return functools.reduce(
            lambda rest, index: jnp.where(into == index, values[index], rest),
            range(1, count),
            values[0],
        )

    def soften(into, source):
        portion = heads // halves if heads % halves == 0 else heads

        def run(base):
            scores = scores_of(into, base)
            for head in range(portion):
                ahead = scores_of(into, base + head + 1) if head + 1 < portion else None
                absorb(into, base + head, scores, source)
                scores = ahead

        if portion == heads:
            run(0)
        else:

            def some(index, carry):
                run(index * portion)
                return carry

            lax.fori_loop(0, heads // portion, some, 0)

    def keep_state():
        for kept, target in zip(state_in, state):
            target[...] = kept[...]

    def wanted(into):
        flag = flag_of(into, 0)
        for at in range(1, group):
            flag = flag | flag_of(into, at)
        return flag

    for at, block in enumerate(blocks):
        lay(block, at)

    def enter(at, carry):
        project(at)
        return carry

    if first:
        project(0)
        soften(0, None)
    elif count == 1:

        @pl.when(wanted(0) != 0)
        def _():
            lax.fori_loop(0, len(blocks), enter, 0)
            soften(0, state_in)

        pl.when(wanted(0) == 0)(keep_state)
    else:
        keep_state()

        def admit(at, carry):
            pl.when(wanted(lax.div(at, group)) != 0)(lambda: project(at))
            return carry

        def turn(into, carry):
            pl.when(wanted(into) != 0)(lambda: soften(into, state))
            return carry

        lax.fori_loop(0, len(blocks), admit, 0)
        lax.fori_loop(0, count, turn, 0)

    if not last:
        tie_ref[...] = sum_ref[0, :8]
    if last:
        lane = lax.broadcasted_iota(jnp.int32, (q_ref.shape[1], 128), 1)
        for head in range(heads):
            total = jnp.sum(sum_ref[head], axis=1, keepdims=True)
            attended_ref[:, head * VDIM : (head + 1) * VDIM] = (acc_ref[head] / total).astype(bf16)
            column = max_ref[head] * score_scale + jnp.log(total)
            logs = column if head == 0 else jnp.where(lane == head, column, logs)
        log_ref[...] = logs.T[:heads]
        for copy in copies:
            copy.wait()
        rows = attended_ref.shape[0] // len(outs)
        for index, out in enumerate(outs):
            start = 0
            if len(outs) == 2:
                start = pl.multiple_of((info[0] if index == 0 else 1 - info[0]) * rows, rows)
            mixed = attended_ref[pl.ds(start, rows), :]
            pooled = pool_ref[pl.ds(start, rows), :]

            def columns(index, carry, out=out, mixed=mixed, pooled=pooled):
                span = pl.ds(pl.multiple_of(index * 1024, 1024), 1024)
                result = dot(mixed, w_attn_ref[:, span]) + dot(pooled, w_pool_ref[:, span])
                out[:, span] = result.astype(out.dtype)
                return carry

            lax.fori_loop(0, out.shape[1] // 1024, columns, 0)


def attn_call(name, info, queries, wk, wv, blocks, group, state, flags, diagonal=False, masked=False, halves=1, tail=None):
    heads, rows, _ = queries.shape
    first, last = state is None, tail is not None
    parts = len(blocks[0])
    keys = blocks[0][0].shape[-1]
    width = group * keys
    total = sum(1 if block[0].ndim == 2 else block[0].shape[0] for block in blocks)
    count = total // group
    body = functools.partial(
        attn_body,
        arrays=len(blocks),
        group=group,
        parts=parts,
        heads=heads,
        first=first,
        last=last,
        diagonal=diagonal,
        masked=masked,
        flags=flags,
        halves=halves,
    )
    operands = [info, queries, wk, wv]
    for block in blocks:
        operands.extend(block)
    specs = [smem_spec] + [vmem_spec] * (len(operands) - 1)
    state_shape = jax.ShapeDtypeStruct((heads, rows, 128), f32)
    aliases = {}
    if not first:
        if not last:
            aliases = {len(operands) + i: i for i in range(3)}
        operands.extend(state)
        specs.extend([vmem_spec] * 3 + [any_spec])
    scratch = [
        pltpu.VMEM((count, heads, NOPE + ROPE, width), bf16),
        pltpu.VMEM((count, heads * VDIM, width), bf16),
        pltpu.VMEM((total, wk.shape[1] + ROPE, keys), bf16),
    ]
    flops = total * keys * heads * 2
    flops = flops * (rows * (NOPE + ROPE + VDIM) + (NOPE + VDIM) * wk.shape[1])
    if last:
        pool_out, w_pool, w_attn = tail
        operands.extend(tail)
        specs.extend([vmem_spec, hbm_spec, hbm_spec])
        model = w_pool.shape[1]
        if parts == 2:
            out_shape = [
                jax.ShapeDtypeStruct((rows // 2, model), f32),
                jax.ShapeDtypeStruct((rows // 2, model), bf16),
            ]
        else:
            out_shape = [jax.ShapeDtypeStruct((rows, model), bf16)]
        out_shape.append(jax.ShapeDtypeStruct((heads, rows), f32))
        scratch = [pltpu.VMEM(state_shape.shape, f32)] * 3 + scratch
        scratch += [
            pltpu.VMEM(w_pool.shape, bf16),
            pltpu.VMEM(w_attn.shape, bf16),
            pltpu.VMEM((rows, heads * VDIM), bf16),
            pltpu.SemaphoreType.DMA((2,)),
        ]
    else:
        out_shape = [state_shape] * 3 + [jax.ShapeDtypeStruct((8, 128), f32)]
    results = pl.pallas_call(
        body,
        name=name,
        out_shape=out_shape,
        in_specs=specs,
        out_specs=[vmem_spec] * len(out_shape),
        scratch_shapes=scratch,
        input_output_aliases=aliases,
        compiler_params=pltpu.CompilerParams(vmem_limit_bytes=40 * 1024 * 1024),
        cost_estimate=pl.CostEstimate(
            flops=flops, bytes_accessed=20 * 1024 * 1024, transcendentals=flops // 600
        ),
    )(*operands)
    return results if last else (results[:3], results[3])


def per_device(
    tokens,
    mix_gain,
    w_pool_in,
    w_qlat,
    w_kvlat,
    w_krope,
    q_gain,
    kv_gain,
    w_q_content,
    w_q_rotary,
    w_key,
    w_value,
    pool_mix,
    pool_scale,
    w_out_pool,
    w_out_attn,
):
    tp_size = lax.axis_size("tp")
    tp_rank = lax.axis_index("tp")
    seq_count = lax.axis_size("sp") // SPAN
    seq_rank = lax.axis_index("sp") // seq_count
    rows, own_width = tokens.shape
    model_width = own_width * tp_size
    pool_cols = w_pool_in.shape[1]
    query_cols = w_qlat.shape[1]
    kv_cols = w_kvlat.shape[1]
    heads = w_key.shape[1] // NOPE
    parts = 2 if tp_size == 2 else 1
    in_plane, plane = seq_rank % PLANE, seq_rank // PLANE

    def swapped(value):
        return lax.ppermute(value, "tp", [(0, 1), (1, 0)])

    def both(value, axis):
        if parts == 2:
            return [value, swapped(value)]
        return [lax.all_gather(value, "tp", axis=axis, tiled=True)]

    def moved(value, keep):
        pairs = [
            (source * seq_count + seq, target * seq_count + seq)
            for source in range(SPAN)
            for target in range(SPAN)
            if keep(source, target)
            for seq in range(seq_count)
        ]
        return lax.ppermute(value, "sp", pairs)

    def by_part(value):
        return value.reshape((parts, value.shape[0] // parts) + value.shape[1:])

    info = jnp.stack(
        [tp_rank, seq_rank, in_plane % 2, in_plane // 2]
        + [(plane >= hop).astype(jnp.int32) for hop in range(1, SPAN // PLANE)]
    ).astype(jnp.int32)
    token_parts = both(tokens, 1)
    in_weights = [w_kvlat, w_krope.T, w_qlat, w_pool_in]
    kv_part, rope_t, query_part, pool_pre = simple_call(
        functools.partial(project_body, parts=parts),
        "project",
        [
            jax.ShapeDtypeStruct((kv_cols, rows), bf16),
            jax.ShapeDtypeStruct((ROPE, rows), f32),
            jax.ShapeDtypeStruct((rows, query_cols), bf16),
            jax.ShapeDtypeStruct((rows, pool_cols), bf16),
        ],
        [info, *token_parts, mix_gain.reshape(parts, 1, model_width // parts), *in_weights],
        2 * 10**9,
        room=60,
    )
    kv_parts = both(kv_part, 0)
    rim = moved(pool_pre[rows - WIDEST :], lambda s, t: t == s + 1)
    query_parts = both(query_part, 1)
    kv_parts[0], seq_rank = lax.optimization_barrier((kv_parts[0], seq_rank))
    positions = (seq_rank * rows + jnp.arange(rows, dtype=jnp.int32)).astype(f32)
    frequency = rope_base ** (-jnp.arange(HALF, dtype=f32) * 2.0 / ROPE)
    angles = frequency[:, None] * positions[None, :]
    cosine, sine = jnp.cos(angles), jnp.sin(angles)
    lane = jnp.arange(128, dtype=jnp.int32)
    lane_frequency = rope_base ** (-(lane % HALF).astype(f32) * 2.0 / ROPE)
    lane_angles = positions[:, None] * lane_frequency[None, :]
    lane_cos = jnp.cos(lane_angles)
    lane_sin = jnp.where(lane % ROPE < HALF, -1.0, 1.0)[None, :] * jnp.sin(lane_angles)

    latent = kv_parts[0].shape[0] * parts
    own_block = simple_call(
        functools.partial(key_body, parts=parts),
        "keys",
        [jax.ShapeDtypeStruct(((latent + ROPE) // parts, rows), bf16)] * parts,
        [info, *kv_parts, rope_t, by_part(kv_gain[:, None]), cosine, sine],
        10**8,
    )

    own_block = list(own_block)
    send = own_block[0]
    x_of = lambda s, t: t == s ^ 1
    y_of = lambda s, t: t == s ^ 2
    rising = lambda rule: lambda s, t: t > s and rule(s, t)
    def with_other(value):
        return [value, swapped(value)] if parts == 2 else [value]

    def step_up(value, hop):
        return moved(value, lambda s, t: t == s + PLANE and s >= PLANE * (hop - 1))

    def within(value, rule, hop):
        return moved(value, lambda s, t: s >= PLANE * hop and rule(s, t))

    hold = lax.optimization_barrier
    near_x, near_y, up1 = moved(send, x_of), moved(send, rising(y_of)), step_up(send, 1)

    own_block[0], w_key, w_value = hold((own_block[0], w_key, w_value))
    wk, wv = simple_call(
        turn_body,
        "turn_weights",
        [jax.ShapeDtypeStruct((weight.shape[1], weight.shape[0]), bf16) for weight in (w_key, w_value)],
        [info, by_part(w_key), by_part(w_value)],
        2 * 10**8,
    )
    queries = simple_call(
        functools.partial(query_body, parts=parts, heads=heads),
        "queries",
        [jax.ShapeDtypeStruct((heads, rows, NOPE + ROPE), bf16)],
        [
            info,
            *query_parts,
            q_gain.reshape(parts, 1, q_gain.shape[0] // parts),
            by_part(w_q_content),
            by_part(w_q_rotary),
            lane_cos,
            lane_sin,
        ],
        6 * 10**8,
    )[0]
    def attend(name, state, blocks, flags, group=2, **options):
        return attn_call(name, info, queries, wk, wv, blocks, group, state, flags, **options)

    flag_x, flag_y, *above = range(2, 3 + SPAN // PLANE)
    above = [None] + above
    state, tie = attend("own", None, [own_block], (), 1, diagonal=True)
    tie, near_x, near_y, up1 = hold((tie, near_x, near_y, up1))
    near = [with_other(near_x), with_other(near_y)]
    far, beside1, up2 = moved(near_x, rising(y_of)), within(up1, x_of, 1), step_up(up1, 2)
    state, tie = attend("near", (*state, tie), near, (flag_x, flag_y), masked=True, halves=2)
    tie, far, up1, beside1, up2, rim = hold((tie, far, up1, beside1, up2, rim))
    ready = [with_other(value) for value in (far, up1, beside1)]
    across = within(stack_pair(up1, up2), y_of, 1)
    beside2, up3 = within(up2, x_of, 2), step_up(up2, 3)
    pool_out = simple_call(
        pool_body,
        "pool",
        [jax.ShapeDtypeStruct((rows, pool_cols), bf16)],
        [
            info,
            pool_pre,
            rim,
            pool_mix,
            pool_scale.reshape(pool_scale.shape[0] // GROUP_DIM, 1, GROUP_DIM),
        ],
        10**8,
    )[0]
    state, tie = attend("up1", (*state, tie), ready, (flag_y, above[1], above[1]), 3, masked=True, halves=2)
    tie, up2, beside2, across, up3 = hold((tie, up2, beside2, across, up3))
    ready = [with_other(value) for value in (up2, beside2, across)]
    corner, across3 = within(across, x_of, 1), within(up3, y_of, 3)
    state, tie = attend("up2", (*state, tie), ready, (above[2], above[2], above[1], above[2]), masked=True, halves=2)
    tie, corner, up3, across3 = hold((tie, corner, up3, across3))
    ready = [with_other(value) for value in (corner, up3, across3)]
    last = within(stack_pair(up3, across3), x_of, 3)
    state, tie = attend("up3", (*state, tie), ready, (above[1], above[2], above[3], above[3]), masked=True, halves=2)
    tie, last = hold((tie, last))
    state = attend(
        "end",
        (*state, tie),
        [with_other(last)],
        (above[3], above[3]),
        tail=(pool_out, w_out_pool, w_out_attn),
    )
    if parts == 2:
        kept, sent, log_total = state
        layer_out = (kept + swapped(sent).astype(f32)).astype(bf16)
    else:
        partial, log_total = state
        layer_out = lax.psum_scatter(partial, "tp", scatter_dimension=0, tiled=True)
    return (layer_out, log_total.T)


def solution(mesh):
    split = P(None, "tp")
    in_specs = (
        P("sp", "tp"),
        P(),
        split,
        split,
        split,
        P(),
        P(),
        P(),
        split,
        split,
        split,
        split,
        P(),
        P(),
        P("tp", None),
        P("tp", None),
    )
    out_specs = (P(("sp", "tp"), None), P("sp", "tp"))
    return jax.shard_map(
        per_device, mesh=mesh, in_specs=in_specs, out_specs=out_specs, check_vma=False
    )
```

```python
import functools

import jax
import jax.numpy as jnp
from jax import lax
from jax.experimental import pallas as pl
from jax.experimental.pallas import tpu as pltpu
from jax.sharding import PartitionSpec as P

NOPE = 128
ROPE = 64
VDIM = 128
GROUP_DIM = 128
WIDEST = 16
SPAN = 16
PLANE = 4
HALF = ROPE // 2
EXTRA = 16

eps_norm = 1e-06
rope_base = 10000.0
masked_score = -1e30
log2e = 1.4426950408889634
score_scale = (NOPE + ROPE) ** (-0.5)


f32, bf16 = jnp.float32, jnp.bfloat16
vmem_spec = pl.BlockSpec(memory_space=pltpu.VMEM)
smem_spec = pl.BlockSpec(memory_space=pltpu.SMEM)
any_spec = pl.BlockSpec(memory_space=pl.ANY)
hbm_spec = pl.BlockSpec(memory_space=pltpu.HBM)


def dot(left, right):
    return jnp.dot(left, right, preferred_element_type=f32)


def slot_of(info, part, parts):
    if parts == 1:
        return 0
    return info[0] if part == 0 else 1 - info[0]


def simple_call(body, name, out_shape, operands, flops, specs=None, scratch=(), room=40):
    specs = specs or [smem_spec] + [vmem_spec] * (len(operands) - 1)
    return pl.pallas_call(
        body,
        name=name,
        out_shape=out_shape,
        in_specs=specs,
        out_specs=[vmem_spec] * len(out_shape),
        scratch_shapes=list(scratch),
        compiler_params=pltpu.CompilerParams(vmem_limit_bytes=room * 1024 * 1024),
        cost_estimate=pl.CostEstimate(
            flops=flops, bytes_accessed=8 * 1024 * 1024, transcendentals=0
        ),
    )(*operands)


def turn_body(info, key_ref, value_ref, key_out, value_out):
    parts, channels, _ = key_ref.shape
    for part in range(parts):
        slot = slot_of(info, part, parts)
        key_out[:, part * channels : (part + 1) * channels] = key_ref[slot].T
        value_out[part * channels : (part + 1) * channels, :] = value_ref[slot]


def project_body(info, *refs, parts):
    tokens = refs[:parts]
    gain, *weights = refs[parts : parts + 5]
    kv_out, rope_out, query_out, pool_out = refs[parts + 5 :]
    squares = None
    scaled = []
    for part in range(parts):
        values = tokens[part][...].astype(f32)
        square = jnp.sum(values * values, axis=1, keepdims=True)
        squares = square if squares is None else squares + square
        scaled.append((values * gain[slot_of(info, part, parts)]).astype(bf16))
    depth = tokens[0].shape[1]
    inverse = lax.rsqrt(squares / (depth * parts) + eps_norm)

    def product(index):
        total = None
        for part in range(parts):
            start = pl.multiple_of(slot_of(info, part, parts) * depth, depth)
            if index == 1:
                piece = lax.dot_general(
                    scaled[part],
                    weights[index][:, pl.ds(start, depth)],
                    (((1,), (1,)), ((), ())),
                    preferred_element_type=f32,
                )
            else:
                piece = dot(scaled[part], weights[index][pl.ds(start, depth), :])
            total = piece if total is None else total + piece
        return (total * inverse).astype(bf16)

    kv_out[...] = product(0).T
    rope = product(1).astype(f32)
    rope_out[...] = jnp.concatenate([rope, jnp.zeros_like(rope)], axis=1).T[:ROPE]
    query_out[...] = product(2)
    pool_out[...] = product(3)


def key_body(info, *refs, parts):
    latents = refs[:parts]
    rope, gain, cosine, sine = refs[parts : parts + 4]
    blocks = refs[parts + 4 :]
    values = [latent[...].astype(f32) for latent in latents]
    squares = sum(jnp.sum(value * value, axis=0, keepdims=True) for value in values)
    channels = values[0].shape[0]
    inverse = lax.rsqrt(squares / (channels * parts) + eps_norm)
    first = rope[:HALF] * cosine[...] - rope[HALF:] * sine[...]
    second = rope[HALF:] * cosine[...] + rope[:HALF] * sine[...]
    for part in range(parts):
        slot = slot_of(info, part, parts)
        blocks[part][:channels] = (values[part] * inverse * gain[slot]).astype(bf16)
        if parts == 1:
            blocks[part][channels : channels + HALF] = first.astype(bf16)
            blocks[part][channels + HALF :] = second.astype(bf16)
        else:
            blocks[part][channels:] = jnp.where(slot == 0, first, second).astype(bf16)


def query_body(info, *refs, parts, heads):
    latents = refs[:parts]
    gain, w_content, w_rotary, cosine, sine, out = refs[parts:]
    values = [latent[...].astype(f32) for latent in latents]
    squares = sum(jnp.sum(value * value, axis=1, keepdims=True) for value in values)
    inverse = lax.rsqrt(squares / (values[0].shape[1] * parts) + eps_norm)
    content = rotary = None
    for part in range(parts):
        slot = slot_of(info, part, parts)
        normed = (values[part] * inverse * gain[slot]).astype(bf16)
        content_part = dot(normed, w_content[slot])
        rotary_part = dot(normed, w_rotary[slot])
        content = content_part if content is None else content + content_part
        rotary = rotary_part if rotary is None else rotary + rotary_part
    lane = lax.broadcasted_iota(jnp.int32, (values[0].shape[0], 128), 1)
    low_half = lane % ROPE < HALF
    for head in range(0, heads, 2):
        raw = rotary[:, head * ROPE : head * ROPE + 128]
        swapped = jnp.where(low_half, pltpu.roll(raw, 128 - HALF, 1), pltpu.roll(raw, HALF, 1))
        turned = raw * cosine[...] + swapped * sine[...]
        out[head, :, NOPE : NOPE + ROPE] = turned[:, :ROPE].astype(bf16)
        out[head + 1, :, NOPE : NOPE + ROPE] = pltpu.roll(turned, ROPE, 1)[:, :ROPE].astype(bf16)
    for head in range(heads):
        out[head, :, :NOPE] = content[:, head * NOPE : (head + 1) * NOPE].astype(bf16)
        out[head, :, NOPE + ROPE :] = jnp.where(lane[:, :EXTRA] == 0, 1.0, 0.0).astype(bf16)


def stack_body(left, right, out):
    out[0], out[1] = left[...], right[...]


def stack_pair(left, right):
    return pl.pallas_call(
        stack_body,
        name="stack_pair",
        out_shape=jax.ShapeDtypeStruct((2,) + left.shape, left.dtype),
        in_specs=[vmem_spec] * 2,
        out_specs=vmem_spec,
        compiler_params=pltpu.CompilerParams(vmem_limit_bytes=8 * 1024 * 1024),
    )(left, right)


def pool_body(info, pool_ref, rim_ref, mix_ref, scale_ref, out_ref):
    rows, cols = pool_ref.shape
    count = cols // GROUP_DIM
    place = lax.broadcasted_iota(jnp.int32, (rows, GROUP_DIM), 0) + info[1] * rows + 1
    for index in range(count):
        span = slice(index * GROUP_DIM, (index + 1) * GROUP_DIM)
        group = info[0] * count + index
        own = pool_ref[:, span].astype(f32)
        total = jnp.concatenate([rim_ref[:, span].astype(f32), own], axis=0)
        stages = []
        for step in (1, 2, 4, 8):
            total = total + pltpu.roll(total, step, 0)
            stages.append(total[WIDEST:])
        if count % 4 == 0:
            window = 2 << (index % 4)
            sums = stages[index % 4]
        else:
            window = jnp.left_shift(jnp.int32(2), group % 4)
            sums = stages[3]
            for stage in range(3):
                sums = jnp.where(group % 4 == stage, stages[stage], sums)
        pooled = sums / jnp.minimum(place, window).astype(f32) - own
        mixed = dot(pooled.astype(bf16), mix_ref[group])
        out_ref[:, span] = (mixed * scale_ref[group]).astype(bf16)


def attn_body(*refs, arrays, group, parts, heads, first, last, diagonal, masked, flags, halves):
    refs = list(refs)
    take = lambda count: [refs.pop(0) for _ in range(count)]
    info, q_ref, wk_ref, wv_ref = take(4)
    blocks = []
    for _ in range(arrays):
        array = take(parts)
        if len(array[0].shape) == 2:
            blocks.append(array)
        else:
            blocks.extend([ref.at[at] for ref in array] for at in range(array[0].shape[0]))
    state_in = take(4)[:3] if not first else None
    if last:
        pool_ref, w_pool_hbm, w_attn_hbm = take(3)
        outs = take(2 if parts == 2 else 1)
        log_ref = refs.pop(0)
        state = take(3)
    else:
        state = take(3)
        tie_ref = refs.pop(0)
    kt_ref, v_ref, lat_ref = take(3)
    max_ref, sum_ref, acc_ref = state
    keys = blocks[0][0].shape[-1]
    factor = score_scale * log2e
    if last:
        w_pool_ref, w_attn_ref, attended_ref, sems = take(4)
        copies = [
            pltpu.make_async_copy(w_attn_hbm, w_attn_ref, sems.at[0]),
            pltpu.make_async_copy(w_pool_hbm, w_pool_ref, sems.at[1]),
        ]
        for copy in copies:
            copy.start()

    count = len(blocks) // group
    width = group * keys

    def lay(block, at):
        channels = block[0].shape[0] - ROPE // parts
        for part in range(parts):
            lat_ref[at, part * channels : (part + 1) * channels] = block[part][:channels, :]
            turn = ROPE // parts
            low = parts * channels + slot_of(info, part, parts) * turn
            lat_ref[at, pl.ds(pl.multiple_of(low, turn), turn)] = block[part][channels:, :]

    def project(at):
        into, place = lax.div(at, group), lax.rem(at, group)
        span = pl.ds(pl.multiple_of(place * keys, 128), keys)
        latent = wk_ref.shape[1]
        bias = jnp.zeros((EXTRA, keys), f32)
        if masked:
            open_block = functools.reduce(
                lambda rest, index: jnp.where(at == index, info[flags[index]], rest),
                range(1, len(flags)),
                info[flags[0]],
            )
            row = lax.broadcasted_iota(jnp.int32, bias.shape, 0)
            bias = jnp.where(row == 0, jnp.where(open_block != 0, 0.0, masked_score), bias)
        bias = bias.astype(bf16)
        k_rows = dot(wk_ref[...], lat_ref[at, :latent]).astype(bf16)
        values = lax.dot_general(
            lat_ref[at, :latent], wv_ref[...], (((0,), (0,)), ((), ())), preferred_element_type=f32
        )
        v_ref[into, pl.ds(pl.multiple_of(place * keys, 128), keys), :] = values.astype(bf16)
        for head in range(heads):
            kt_ref[into, head, :NOPE, span] = k_rows[head * NOPE : (head + 1) * NOPE]
            kt_ref[into, head, NOPE : NOPE + ROPE, span] = lat_ref[at, latent:]
            kt_ref[into, head, NOPE + ROPE :, span] = bias

    def scores_of(into, head):
        return dot(q_ref[head], kt_ref[into, head])

    def absorb(into, head, scores, source):
        tiles = [scores[:, tile * 128 : (tile + 1) * 128] for tile in range(width // 128)]
        if diagonal:
            row = lax.broadcasted_iota(jnp.int32, tiles[0].shape, 0)
            col = lax.broadcasted_iota(jnp.int32, tiles[0].shape, 1)
            tiles = [
                jnp.where(col + tile * 128 <= row, value, masked_score)
                for tile, value in enumerate(tiles)
            ]
        peak = functools.reduce(jnp.maximum, tiles)
        peak = jnp.max(peak, axis=1, keepdims=True)
        if source is None:
            new = jnp.broadcast_to(peak, tiles[0].shape)
            total = None
        else:
            old = source[0][head]
            new = jnp.maximum(old, peak)
            shrink = jnp.exp2((old - new) * factor)
            total = source[1][head] * shrink
        weights = []
        for value in tiles:
            expo = jnp.exp2((value - new) * factor)
            total = expo if total is None else total + expo
            weights.append(expo.astype(bf16))
        column = pl.ds(pl.multiple_of(head * VDIM, VDIM), VDIM)
        update = dot(jnp.concatenate(weights, axis=1), v_ref[into, :, column])
        max_ref[head] = new
        sum_ref[head] = total
        acc_ref[head] = update if source is None else source[2][head] * shrink + update

    def flag_of(into, at):
        if isinstance(into, int):
            return info[flags[into * group + at]]
        values = [info[flags[index * group + at]] for index in range(count)]
        return functools.reduce(
            lambda rest, index: jnp.where(into == index, values[index], rest),
            range(1, count),
            values[0],
        )

    def soften(into, source):
        portion = heads // halves if heads % halves == 0 else heads

        def run(base):
            scores = scores_of(into, base)
            for head in range(portion):
                ahead = scores_of(into, base + head + 1) if head + 1 < portion else None
                absorb(into, base + head, scores, source)
                scores = ahead

        if portion == heads:
            run(0)
        else:

            def some(index, carry):
                run(index * portion)
                return carry

            lax.fori_loop(0, heads // portion, some, 0)

    def keep_state():
        for kept, target in zip(state_in, state):
            target[...] = kept[...]

    def wanted(into):
        flag = flag_of(into, 0)
        for at in range(1, group):
            flag = flag | flag_of(into, at)
        return flag

    for at, block in enumerate(blocks):
        lay(block, at)

    def enter(at, carry):
        project(at)
        return carry

    if first:
        project(0)
        soften(0, None)
    elif count == 1:

        @pl.when(wanted(0) != 0)
        def _():
            lax.fori_loop(0, len(blocks), enter, 0)
            soften(0, state_in)

        pl.when(wanted(0) == 0)(keep_state)
    else:
        keep_state()

        def admit(at, carry):
            pl.when(wanted(lax.div(at, group)) != 0)(lambda: project(at))
            return carry

        def turn(into, carry):
            pl.when(wanted(into) != 0)(lambda: soften(into, state))
            return carry

        lax.fori_loop(0, len(blocks), admit, 0)
        lax.fori_loop(0, count, turn, 0)

    if not last:
        tie_ref[...] = sum_ref[0, :8]
    if last:
        lane = lax.broadcasted_iota(jnp.int32, (q_ref.shape[1], 128), 1)
        for head in range(heads):
            total = jnp.sum(sum_ref[head], axis=1, keepdims=True)
            share = acc_ref[head] * (1.0 / total)
            attended_ref[:, head * VDIM : (head + 1) * VDIM] = share.astype(bf16)
            column = max_ref[head] * score_scale + jnp.log(total)
            logs = column if head == 0 else jnp.where(lane == head, column, logs)
        log_ref[...] = logs.T[:heads]
        for copy in copies:
            copy.wait()
        rows = attended_ref.shape[0] // len(outs)

        def columns(index, carry):
            span = pl.ds(pl.multiple_of(index * 512, 512), 512)
            result = dot(attended_ref[...], w_attn_ref[:, span])
            result = result + dot(pool_ref[...], w_pool_ref[:, span])
            if len(outs) == 1:
                outs[0][:, span] = result.astype(outs[0].dtype)
            else:
                top, bottom = result[:rows], result[rows:]
                kept, sent = outs
                kept[:, span] = jnp.where(info[0] == 0, top, bottom)
                sent[:, span] = jnp.where(info[0] == 0, bottom, top).astype(sent.dtype)
            return carry

        lax.fori_loop(0, outs[0].shape[1] // 512, columns, 0)


def attn_call(name, info, queries, wk, wv, blocks, group, state, flags, diagonal=False, masked=False, halves=1, tail=None):
    heads, rows, _ = queries.shape
    first, last = state is None, tail is not None
    parts = len(blocks[0])
    keys = blocks[0][0].shape[-1]
    width = group * keys
    total = sum(1 if block[0].ndim == 2 else block[0].shape[0] for block in blocks)
    count = total // group
    body = functools.partial(
        attn_body,
        arrays=len(blocks),
        group=group,
        parts=parts,
        heads=heads,
        first=first,
        last=last,
        diagonal=diagonal,
        masked=masked,
        flags=flags,
        halves=halves,
    )
    operands = [info, queries, wk, wv]
    for block in blocks:
        operands.extend(block)
    specs = [smem_spec] + [vmem_spec] * (len(operands) - 1)
    state_shape = jax.ShapeDtypeStruct((heads, rows, 128), f32)
    aliases = {}
    if not first:
        if not last:
            aliases = {len(operands) + i: i for i in range(3)}
        operands.extend(state)
        specs.extend([vmem_spec] * 3 + [any_spec])
    scratch = [
        pltpu.VMEM((count, heads, NOPE + ROPE + EXTRA, width), bf16),
        pltpu.VMEM((count, width, heads * VDIM), bf16),
        pltpu.VMEM((total, wk.shape[1] + ROPE, keys), bf16),
    ]
    flops = total * keys * heads * 2
    flops = flops * (rows * (NOPE + ROPE + VDIM) + (NOPE + VDIM) * wk.shape[1])
    if last:
        pool_out, w_pool, w_attn = tail
        operands.extend(tail)
        specs.extend([vmem_spec, hbm_spec, hbm_spec])
        model = w_pool.shape[1]
        if parts == 2:
            out_shape = [
                jax.ShapeDtypeStruct((rows // 2, model), f32),
                jax.ShapeDtypeStruct((rows // 2, model), bf16),
            ]
        else:
            out_shape = [jax.ShapeDtypeStruct((rows, model), bf16)]
        out_shape.append(jax.ShapeDtypeStruct((heads, rows), f32))
        scratch = [pltpu.VMEM(state_shape.shape, f32)] * 3 + scratch
        scratch += [
            pltpu.VMEM(w_pool.shape, bf16),
            pltpu.VMEM(w_attn.shape, bf16),
            pltpu.VMEM((rows, heads * VDIM), bf16),
            pltpu.SemaphoreType.DMA((2,)),
        ]
    else:
        out_shape = [state_shape] * 3 + [jax.ShapeDtypeStruct((8, 128), f32)]
    results = pl.pallas_call(
        body,
        name=name,
        out_shape=out_shape,
        in_specs=specs,
        out_specs=[vmem_spec] * len(out_shape),
        scratch_shapes=scratch,
        input_output_aliases=aliases,
        compiler_params=pltpu.CompilerParams(vmem_limit_bytes=40 * 1024 * 1024),
        cost_estimate=pl.CostEstimate(
            flops=flops, bytes_accessed=20 * 1024 * 1024, transcendentals=flops // 600
        ),
    )(*operands)
    return results if last else (results[:3], results[3])


def per_device(
    tokens,
    mix_gain,
    w_pool_in,
    w_qlat,
    w_kvlat,
    w_krope,
    q_gain,
    kv_gain,
    w_q_content,
    w_q_rotary,
    w_key,
    w_value,
    pool_mix,
    pool_scale,
    w_out_pool,
    w_out_attn,
):
    tp_size = lax.axis_size("tp")
    tp_rank = lax.axis_index("tp")
    seq_count = lax.axis_size("sp") // SPAN
    seq_rank = lax.axis_index("sp") // seq_count
    rows, own_width = tokens.shape
    model_width = own_width * tp_size
    pool_cols = w_pool_in.shape[1]
    query_cols = w_qlat.shape[1]
    kv_cols = w_kvlat.shape[1]
    heads = w_key.shape[1] // NOPE
    parts = 2 if tp_size == 2 else 1
    in_plane, plane = seq_rank % PLANE, seq_rank // PLANE

    def swapped(value):
        return lax.ppermute(value, "tp", [(0, 1), (1, 0)])

    def both(value, axis):
        if parts == 2:
            return [value, swapped(value)]
        return [lax.all_gather(value, "tp", axis=axis, tiled=True)]

    def moved(value, keep):
        pairs = [
            (source * seq_count + seq, target * seq_count + seq)
            for source in range(SPAN)
            for target in range(SPAN)
            if keep(source, target)
            for seq in range(seq_count)
        ]
        return lax.ppermute(value, "sp", pairs)

    def by_part(value):
        return value.reshape((parts, value.shape[0] // parts) + value.shape[1:])

    info = jnp.stack(
        [tp_rank, seq_rank, in_plane % 2, in_plane // 2]
        + [(plane >= hop).astype(jnp.int32) for hop in range(1, SPAN // PLANE)]
    ).astype(jnp.int32)
    token_parts = both(tokens, 1)
    in_weights = [w_kvlat, w_krope.T, w_qlat, w_pool_in]
    kv_part, rope_t, query_part, pool_pre = simple_call(
        functools.partial(project_body, parts=parts),
        "project",
        [
            jax.ShapeDtypeStruct((kv_cols, rows), bf16),
            jax.ShapeDtypeStruct((ROPE, rows), f32),
            jax.ShapeDtypeStruct((rows, query_cols), bf16),
            jax.ShapeDtypeStruct((rows, pool_cols), bf16),
        ],
        [info, *token_parts, mix_gain.reshape(parts, 1, model_width // parts), *in_weights],
        2 * 10**9,
        room=60,
    )
    kv_parts = both(kv_part, 0)
    rim_rows = pool_pre[rows - WIDEST :]
    query_parts = both(query_part, 1)
    kv_parts[0], seq_rank = lax.optimization_barrier((kv_parts[0], seq_rank))
    positions = (seq_rank * rows + jnp.arange(rows, dtype=jnp.int32)).astype(f32)
    frequency = rope_base ** (-jnp.arange(HALF, dtype=f32) * 2.0 / ROPE)
    angles = frequency[:, None] * positions[None, :]
    cosine, sine = jnp.cos(angles), jnp.sin(angles)
    lane = jnp.arange(128, dtype=jnp.int32)
    lane_frequency = rope_base ** (-(lane % HALF).astype(f32) * 2.0 / ROPE)
    lane_angles = positions[:, None] * lane_frequency[None, :]
    lane_cos = jnp.cos(lane_angles)
    lane_sin = jnp.where(lane % ROPE < HALF, -1.0, 1.0)[None, :] * jnp.sin(lane_angles)

    latent = kv_parts[0].shape[0] * parts
    own_block = simple_call(
        functools.partial(key_body, parts=parts),
        "keys",
        [jax.ShapeDtypeStruct(((latent + ROPE) // parts, rows), bf16)] * parts,
        [info, *kv_parts, rope_t, by_part(kv_gain[:, None]), cosine, sine],
        10**8,
    )

    own_block = list(own_block)
    send = own_block[0]
    x_of = lambda s, t: t == s ^ 1
    y_of = lambda s, t: t == s ^ 2
    rising = lambda rule: lambda s, t: t > s and rule(s, t)
    def with_other(value):
        return [value, swapped(value)] if parts == 2 else [value]

    def step_up(value, hop):
        return moved(value, lambda s, t: t == s + PLANE and s >= PLANE * (hop - 1))

    def within(value, rule, hop):
        return moved(value, lambda s, t: s >= PLANE * hop and rule(s, t))

    hold = lax.optimization_barrier
    near_x, near_y, up1 = moved(send, x_of), moved(send, rising(y_of)), step_up(send, 1)

    own_block[0], w_key, w_value = hold((own_block[0], w_key, w_value))
    wk, wv = simple_call(
        turn_body,
        "turn_weights",
        [jax.ShapeDtypeStruct(w_key.shape[::-1], bf16), jax.ShapeDtypeStruct(w_value.shape, bf16)],
        [info, by_part(w_key), by_part(w_value)],
        2 * 10**8,
    )
    queries = simple_call(
        functools.partial(query_body, parts=parts, heads=heads),
        "queries",
        [jax.ShapeDtypeStruct((heads, rows, NOPE + ROPE + EXTRA), bf16)],
        [
            info,
            *query_parts,
            q_gain.reshape(parts, 1, q_gain.shape[0] // parts),
            by_part(w_q_content),
            by_part(w_q_rotary),
            lane_cos,
            lane_sin,
        ],
        6 * 10**8,
    )[0]
    def attend(name, state, blocks, flags, group=2, **options):
        return attn_call(name, info, queries, wk, wv, blocks, group, state, flags, **options)

    flag_x, flag_y, *above = range(2, 3 + SPAN // PLANE)
    above = [None] + above
    state, tie = attend("own", None, [own_block], (), 1, diagonal=True)
    tie, near_x, near_y, up1 = hold((tie, near_x, near_y, up1))
    near = [with_other(near_x), with_other(near_y)]
    far, beside1, up2 = moved(near_x, rising(y_of)), within(up1, x_of, 1), step_up(up1, 2)
    state, tie = attend("near", (*state, tie), near, (flag_x, flag_y), masked=True)
    tie, far, up1, beside1, up2 = hold((tie, far, up1, beside1, up2))
    ready = [with_other(value) for value in (far, up1, beside1)]
    across = within(stack_pair(up1, up2), y_of, 1)
    beside2, up3 = within(up2, x_of, 2), step_up(up2, 3)
    state, tie = attend("up1", (*state, tie), ready, (flag_y, above[1], above[1]), 3, masked=True, halves=2)
    tie, up2, beside2, across, up3 = hold((tie, up2, beside2, across, up3))
    ready = [with_other(value) for value in (up2, beside2, across)]
    corner, across3 = within(across, x_of, 1), within(up3, y_of, 3)
    state, tie = attend("up2", (*state, tie), ready, (above[2], above[2], above[1], above[2]), masked=True, halves=2)
    tie, corner, up3, across3, rim_rows = hold((tie, corner, up3, across3, rim_rows))
    ready = [with_other(value) for value in (corner, up3, across3)]
    last = within(stack_pair(up3, across3), x_of, 3)
    rim = moved(rim_rows, lambda s, t: t == s + 1)
    state, tie = attend("up3", (*state, tie), ready, (above[1], above[2], above[3], above[3]), masked=True, halves=2)
    tie, last, rim = hold((tie, last, rim))
    pool_out = simple_call(
        pool_body,
        "pool",
        [jax.ShapeDtypeStruct((rows, pool_cols), bf16)],
        [
            info,
            pool_pre,
            rim,
            pool_mix,
            pool_scale.reshape(pool_scale.shape[0] // GROUP_DIM, 1, GROUP_DIM),
        ],
        10**8,
    )[0]
    state = attend(
        "end",
        (*state, tie),
        [with_other(last)],
        (above[3], above[3]),
        tail=(pool_out, w_out_pool, w_out_attn),
    )
    if parts == 2:
        kept, sent, log_total = state
        layer_out = (kept + swapped(sent).astype(f32)).astype(bf16)
    else:
        partial, log_total = state
        layer_out = lax.psum_scatter(partial, "tp", scatter_dimension=0, tiled=True)
    return (layer_out, log_total.T)


def solution(mesh):
    split = P(None, "tp")
    in_specs = (
        P("sp", "tp"),
        P(),
        split,
        split,
        split,
        P(),
        P(),
        P(),
        split,
        split,
        split,
        split,
        P(),
        P(),
        P("tp", None),
        P("tp", None),
    )
    out_specs = (P(("sp", "tp"), None), P("sp", "tp"))
    return jax.shard_map(
        per_device, mesh=mesh, in_specs=in_specs, out_specs=out_specs, check_vma=False
    )
```
